512 devices in a mesh: grp: 2 (over y), ra: 32 (over z), cb: 8 (over x, core).
Axes of the slice: x: 4, y: 2, z: 32, core: 2. Of those that a mesh axis runs over, the one named last changes fastest.
The devices are a block of a 4x8x32 slice.
Arguments:
- tokens: bfloat16 [512, 4096], P('grp', 'cb'), parts along dimension 0, may hold values from -50 to 50
- norm_gains: float32 [3, 4096], P(None, 'cb'), may hold values from 0.1 to 1.9
- gate_weight: float32 [2, 4096, 11264], P(None, 'cb', 'ra'), may hold values from -0.09375 to 0.09375
- value_weight: float32 [2, 4096, 11264], P(None, 'cb', 'ra'), may hold values from -0.09375 to 0.09375
- gate_scale: float32 [2, 11264], P(None, 'ra'), may hold values from 0.3 to 3
- value_scale: float32 [2, 11264], P(None, 'ra'), may hold values from 0.3 to 3
- conv_gate: float32 [2, 3, 11264], P(None, None, 'ra'), may hold values from -3 to 3
- conv_value: float32 [2, 3, 11264], P(None, None, 'ra'), may hold values from -3 to 3
- down_weight: float32 [2, 11264, 4096], P(None, 'ra', 'cb'), may hold values from -0.07537784 to 0.07537784
- down_scale: float32 [2, 4096], P(None, 'cb'), may hold values from 0.3 to 3
Outputs:
- normed_out: bfloat16 [512, 4096], P('grp', 'cb'), parts along dimension 0
The draws below stay inside these ranges and needn't reach their ends.
There are 2 independent parts, one for each index of `grp`. The reference program is written for one: setup_inputs(seed, part) draws one part's arguments, and reference() takes and returns one part's arrays. A program takes and returns all parts, laid end to end along the dimension named above; an argument that names none is the same for every part. Nothing has to cross between parts.
All inputs are finite; a program needn't handle non-finite values.
Results may differ from the reference program's by a relative error of at most 0.012.
The reference program's roundings to bfloat16 on the way count: a program that leaves them out, or rounds other values in their place, can miss the bound.
Values may be sent and summed in bfloat16 or wider, within the bound.
A program may use at most 64 MiB of HBM per device.

```python
import math
import jax
import jax.numpy as jnp
from jax import lax

D = 4096
FF = 11264
TOK = 256
LAYERS = 2
TAPS = 3


def draw_tokens(key, part):
    key_values = jax.random.fold_in(key, 11)
    key_rows = jax.random.fold_in(key, 12)
    col_position = jnp.arange(D, dtype=jnp.float32) / D
    col_scale = 10.0 ** (col_position - 0.5)
    row_scale = 10.0 ** (jax.random.uniform(key_rows, (TOK, 1), jnp.float32) - 0.5)
    values = jnp.clip(jax.random.normal(key_values, (TOK, D), jnp.float32), -5.0, 5.0)
    return (values * row_scale * col_scale).astype(jnp.bfloat16)


def draw_down_weight(key, part):
    key_base = jax.random.fold_in(key, 21)
    unit = FF ** (-0.5)
    base = jnp.clip(jax.random.normal(key_base, (LAYERS, FF, D), jnp.float32), -6.0, 6.0) * unit
    values = base
    return values.astype(jnp.float32)


def steps_of(rng, dims, shards, least, largest):
    loudness = 1.0
    for axis_at, parts in shards:
        heights = jax.random.uniform(jax.random.fold_in(jax.random.fold_in(rng, 6), axis_at), (parts,), jnp.float32, least / len(shards), largest / len(shards))
        loudness = loudness * jnp.repeat(jnp.exp(heights), dims[axis_at] // parts).reshape((-1,) + (1,) * (len(dims) - 1 - axis_at))
    return loudness


def centred(own_key, dims, scale, bound, shards=(), kind=jnp.bfloat16):
    drawn = jax.random.normal(own_key, dims, jnp.float32) * scale
    if len(shards) > 0:
        drawn = steps_of(own_key, dims, shards, -0.22, 0.18) * drawn
    return jnp.clip(drawn, min=-bound, max=bound).astype(kind)


def setup_inputs(seed: int = 0, part: int = 0) -> dict:
    streams_of = jax.random.split(jax.random.key(seed), 11)
    own_keys = jax.random.split(jax.random.fold_in(streams_of[10], part), 11)
    return {
        "tokens": draw_tokens(jax.random.fold_in(jax.random.fold_in(streams_of[10], part), 71), part),
        "norm_gains": jnp.clip(1.0 + 0.18 * jax.random.normal(streams_of[1], (LAYERS + 1, D), jnp.float32), 0.1, 1.9),
        "gate_weight": centred(streams_of[2], (LAYERS, D, FF), D ** -0.5, 0.09375, ((1, 8), (2, 32)), jnp.float32),
        "value_weight": centred(streams_of[3], (LAYERS, D, FF), D ** -0.5, 0.09375, ((1, 8), (2, 32)), jnp.float32),
        "gate_scale": jnp.clip(jnp.exp(math.log(3.0) - 2.3025851 * jax.random.uniform(streams_of[4], (LAYERS, FF), jnp.float32) ** steps_of(streams_of[4], (LAYERS, FF), ((1, 32),), -0.2, 0.2)), 0.3, 3.0),
        "value_scale": jnp.clip(jnp.exp(math.log(3.0) - 2.3025851 * jax.random.uniform(streams_of[5], (LAYERS, FF), jnp.float32) ** steps_of(streams_of[5], (LAYERS, FF), ((1, 32),), -0.2, 0.2)), 0.3, 3.0),
        "conv_gate": centred(streams_of[6], (LAYERS, TAPS, FF), 0.6, 3.0, ((2, 32),), jnp.float32),
        "conv_value": centred(streams_of[7], (LAYERS, TAPS, FF), 0.6, 3.0, ((2, 32),), jnp.float32),
        "down_weight": draw_down_weight(jax.random.fold_in(streams_of[10], 71), part),
        "down_scale": jnp.clip(jnp.exp(math.log(3.0) - 2.3025851 * jax.random.uniform(streams_of[9], (LAYERS, D), jnp.float32) ** steps_of(streams_of[9], (LAYERS, D), ((1, 8),), -0.2, 0.2)), 0.3, 3.0),
    }


epsilon = 1e-06
residual_weight = 0.5

def rms_scale(values):
    return lax.rsqrt(lax.optimization_barrier(jnp.mean(values * values, axis=1, keepdims=True)) + epsilon)

def causal_taps(projected, tap_weights):
    tap_count = tap_weights.shape[0]
    row_count = projected.shape[0]
    padded = jnp.pad(projected, ((tap_count - 1, 0), (0, 0)))
    result = jnp.zeros_like(projected)
    for tap_idx in range(tap_count):
        result = result + padded[tap_idx:tap_idx + row_count] * tap_weights[tap_idx]
    return result

def reference(tokens, norm_gains, gate_weight, value_weight, gate_scale, value_scale, conv_gate, conv_value, down_weight, down_scale):
    current = tokens
    for layer_idx in range(LAYERS):
        state_wide = current.astype(jnp.float32)
        inverse = rms_scale(state_wide)
        scaled = (state_wide * norm_gains[layer_idx]).astype(jnp.bfloat16)
        gate_pre = inverse * gate_scale[layer_idx] * jnp.dot(scaled, gate_weight[layer_idx].astype(jnp.bfloat16), preferred_element_type=jnp.float32)
        value_pre = inverse * value_scale[layer_idx] * jnp.dot(scaled, value_weight[layer_idx].astype(jnp.bfloat16), preferred_element_type=jnp.float32)
        hidden = (jax.nn.gelu(causal_taps(gate_pre, conv_gate[layer_idx]), approximate=True) * causal_taps(value_pre, conv_value[layer_idx])).astype(jnp.bfloat16)
        down_total = jnp.dot(hidden, down_weight[layer_idx].astype(jnp.bfloat16), preferred_element_type=jnp.float32)
        current = (residual_weight * state_wide + down_scale[layer_idx] * down_total).astype(jnp.bfloat16)
    state_wide = current.astype(jnp.float32)
    return (state_wide * rms_scale(state_wide) * norm_gains[LAYERS]).astype(jnp.bfloat16)
```

```python
import functools

import jax
import jax.numpy as jnp
from jax import lax
from jax.experimental import pallas as pl
from jax.experimental.pallas import tpu as pltpu
from jax.sharding import PartitionSpec as P

epsilon = 1e-06
residual_weight = 0.5
MESH = pl.DeviceIdType.MESH
f32 = jnp.float32
bf16 = jnp.bfloat16


def in_three(column):
    hi = column.astype(bf16).astype(f32)
    mid = (column - hi).astype(bf16).astype(f32)
    lo = (column - hi - mid).astype(bf16).astype(f32)
    return hi, mid, lo


def with_lanes(tile, at, columns):
    lane = lax.broadcasted_iota(jnp.int32, tile.shape, 1)
    for k, column in enumerate(columns):
        tile = jnp.where(lane == at + k, column, tile)
    return tile


def kernel(
    dims,
    tok,
    gains,
    gate_w,
    value_w,
    gate_scale,
    value_scale,
    conv_gate,
    conv_value,
    down_w,
    down_scale,
    out,
    raw_in,
    raw_down,
    w_in,
    w_down,
    part,
    part_halo,
    got,
    got_halo,
    pre,
    hid,
    down_part,
    win,
    sums,
    cur,
    norm,
    w_sem,
    ps,
    pr,
    qs,
    qr,
    gs,
    gr,
    zs,
    zr,
    ms,
    mr,
    bs,
    br,
    ns,
    nr,
):
    layers, nz, nc, width, ff, ffp, blk, taps = dims
    owners = nz // nc
    half = nc // 2
    halo = taps - 1
    model_width = width * nc
    z = lax.axis_index("ra")
    c = lax.axis_index("cb")
    mine = lax.rem(z, nc)
    rank = z // nc

    def along_z(d):
        return {"ra": lax.rem(z + d + 2 * nz, nz), "cb": c}

    def along_c(k):
        return {"ra": z, "cb": lax.rem(c + k, nc)}

    def send(src, dst, ssem, rsem, to):
        return pltpu.make_async_remote_copy(
            src_ref=src, dst_ref=dst, send_sem=ssem, recv_sem=rsem, device_id=to, device_id_type=MESH
        )

    loads = []
    for layer in range(layers):
        for k, (src, dst) in enumerate(
            ((gate_w, raw_in.at[layer, 0]), (value_w, raw_in.at[layer, 1]), (down_w, raw_down.at[layer]))
        ):
            load = pltpu.make_async_copy(src.at[layer], dst, w_sem.at[layer, k])
            load.start()
            loads.append(load)

    barrier = pltpu.get_barrier_semaphore()
    peers = [along_c(k) for k in range(1, nc)]
    peers += [along_z(d) for d in range(-half, half + 1) if d != 0]
    peers += [along_z(nc * j) for j in range(1, owners)]
    for to in peers:
        pl.semaphore_signal(barrier, inc=1, device_id=to, device_id_type=MESH)

    edge = ff // 128 * 128
    for layer in range(layers):
        for s in range(2):
            w_in[layer, :, s * ffp + edge : (s + 1) * ffp] = jnp.zeros((width, ffp - edge), bf16)
        w_down[layer, ff:, :] = jnp.zeros((ffp - ff, width), bf16)
        part_halo[layer, 0] = jnp.zeros((halo, 2 * ffp), bf16)
        hid[layer, c, :, edge:] = jnp.zeros((blk, ffp - edge), bf16)

    def take_weights(layer):
        for load in loads[3 * layer : 3 * layer + 3]:
            load.wait()
        w_in[layer, :, 0:ff] = raw_in[layer, 0].astype(bf16)
        w_in[layer, :, ffp : ffp + ff] = raw_in[layer, 1].astype(bf16)
        w_down[layer, 0:ff, :] = raw_down[layer].astype(bf16)

    def partials(x, layer):
        scaled = (x * gains[layer : layer + 1, :]).astype(bf16)
        p = jnp.dot(scaled, w_in[layer], preferred_element_type=f32)
        squares = in_three(jnp.sum(x * x, axis=1, keepdims=True))
        last = with_lanes(p[:, edge:ffp], ff - edge, squares)
        return jnp.concatenate([p[:, :edge], last, p[:, ffp:]], axis=1)

    def part_copy(layer, b, src):
        return send(part.at[layer, b], got.at[layer, src], ps.at[layer, b], pr.at[layer, src], {"ra": z, "cb": b})

    def halo_copy(layer, b, src):
        return send(
            part_halo.at[layer, b], got_halo.at[layer, src], qs.at[layer, b], qr.at[layer, src], {"ra": z, "cb": b}
        )

    def hid_copy(layer, b, to):
        return send(
            hid.at[layer, b], hid.at[layer, b], gs.at[layer, to], gr.at[layer, b], {"ra": z, "cb": to}
        )

    def win_copy(layer, b, slot):
        return send(
            down_part.at[layer, b], win.at[layer, slot], zs.at[layer, b], zr.at[layer, slot], along_z(slot - (half - 1))
        )

    def sum_copy(layer, k, j):
        return send(sums.at[layer, k], sums.at[layer, k], ms.at[layer, j], mr.at[layer, k], along_z(nc * j))

    def cur_copy(layer, b, slot):
        return send(
            cur.at[layer, b], cur.at[layer, b], bs.at[layer, slot], br.at[layer, slot], along_z(half - 1 - slot)
        )

    def norm_copy(b, to):
        return send(norm.at[b], norm.at[b], ns.at[to], nr.at[b], {"ra": z, "cb": to})

    def near_first(i):
        return (2 * lax.rem(i, 2) - 1) * ((i + 1) // 2)

    for layer in range(layers):
        take_weights(layer) if layer == 0 else None
        if layer == 0:
            p = partials(tok[...].astype(f32), 0).reshape(nc, blk, 2 * ffp)
            part[0] = p.astype(bf16)
            for b in range(1, nc):
                part_halo[0, b] = p[b - 1, blk - halo :, :].astype(bf16)
            pl.semaphore_wait(barrier, len(peers))
            for k in (4, 3, 5, 2, 6, 1, 7) if nc == 8 else range(1, nc):
                to = lax.rem(c + k, nc)
                part_copy(0, to, c).start()
                halo_copy(0, to, c).start()
        else:

            def one_block(i, carry, layer=layer):
                d = near_first(i)
                b = lax.rem(z + d + nz, nc)
                slot = d + (half - 1)

                @pl.when(i > 0)
                def _():
                    cur_copy(layer - 1, b, slot).wait_recv()

                p = partials(cur[layer - 1, b].astype(f32), layer)
                part[layer, b] = p.astype(bf16)

                @pl.when(b != c)
                def _():
                    part_copy(layer, b, c).start()

                after = lax.rem(b + 1, nc)

                @pl.when(after != 0)
                def _():
                    part_halo[layer, after] = p[blk - halo :, :].astype(bf16)

                @pl.when(after != c)
                def _():
                    halo_copy(layer, after, c).start()

                return carry

            lax.fori_loop(0, nc, one_block, 0)

        got[layer, c] = part[layer, c]
        got_halo[layer, c] = part_halo[layer, c]
        if layer + 1 < layers:
            take_weights(layer + 1)
        for k in range(1, nc):
            src = lax.rem(c + k, nc)
            part_copy(layer, c, src).wait_recv()
            halo_copy(layer, c, src).wait_recv()
        for buf, rows, at in ((got_halo, halo, 8 - halo), (got, blk, 8)):
            total = buf[layer, 0].astype(f32)
            for src in range(1, nc):
                total = total + buf[layer, src].astype(f32)
            squares = jnp.sum(total[:, ff : ff + 3], axis=1, keepdims=True)
            inverse = lax.rsqrt(squares / model_width + epsilon)
            pre[at : at + rows, 0:ff] = inverse * gate_scale[layer : layer + 1, :] * total[:, 0:ff]
            pre[at : at + rows, ffp : ffp + ff] = (
                inverse * value_scale[layer : layer + 1, :] * total[:, ffp : ffp + ff]
            )
        convs = []
        for lane, weights in ((0, conv_gate), (ffp, conv_value)):
            y = None
            for k in range(taps):
                term = pre[8 - halo + k : 8 - halo + k + blk, lane : lane + ff] * weights[layer, k : k + 1, :]
                y = term if y is None else y + term
            convs.append(y)
        hid[layer, c, :, 0:ff] = (jax.nn.gelu(convs[0], approximate=True) * convs[1]).astype(bf16)
        for k in (4, 3, 5, 2, 6, 1, 7) if nc == 8 else range(1, nc):
            hid_copy(layer, c, lax.rem(c + k, nc)).start()

        def down_block(i, carry, layer=layer):
            b = lax.rem(c + near_first(i) + nc, nc)

            @pl.when(i > 0)
            def _():
                hid_copy(layer, b, c).wait_recv()

            down_part[layer, b] = jnp.dot(hid[layer, b], w_down[layer], preferred_element_type=f32).astype(bf16)
            slot = lax.rem(b - z + (half - 1) + nz, nc)

            @pl.when(slot != half - 1)
            def _():
                win_copy(layer, b, slot).start()

            return carry

        lax.fori_loop(0, nc, down_block, 0)

        win[layer, half - 1] = down_part[layer, mine]
        for slot in range(nc):
            if slot != half - 1:
                win_copy(layer, mine, slot).wait_recv()
        total = win[layer, 0].astype(f32)
        for slot in range(1, nc):
            total = total + win[layer, slot].astype(f32)
        sums[layer, rank] = total.astype(bf16)
        far_first = sorted(range(1, owners), key=lambda j: -min(j, owners - j))
        for j in far_first:
            sum_copy(layer, rank, j).start()
        for j in far_first:
            sum_copy(layer, lax.rem(rank + j, owners), j).wait_recv()
        total = sums[layer, 0].astype(f32)
        for k in range(1, owners):
            total = total + sums[layer, k].astype(f32)
        if layer == 0:
            own = tok[pl.ds(pl.multiple_of(mine * blk, blk), blk), :].astype(f32)
        else:
            own = cur[layer - 1, mine].astype(f32)
        new = (residual_weight * own + down_scale[layer : layer + 1, :] * total).astype(bf16)

        if layer == layers - 1:
            wide = new.astype(f32)
            squares = in_three(jnp.sum(wide * wide, axis=1, keepdims=True))
            norm[c] = with_lanes(jnp.zeros((blk, 128), f32), 0, squares).astype(bf16)
            for k in range(1, nc):
                norm_copy(c, lax.rem(c + k, nc)).start()
            for k in range(1, nc):
                norm_copy(lax.rem(c + k, nc), c).wait_recv()
            both = norm[0].astype(f32)
            for k in range(1, nc):
                both = both + norm[k].astype(f32)
            squares = jnp.sum(both[:, 0:3], axis=1, keepdims=True)
            inverse = lax.rsqrt(squares / model_width + epsilon)
            new = (wide * inverse * gains[layers : layers + 1, :]).astype(bf16)
        cur[layer, mine] = new
        for slot in range(nc):
            if slot != half - 1:
                cur_copy(layer, mine, slot).start()

    last = layers - 1

    def put_block(i, carry):
        d = near_first(i)
        b = lax.rem(z + d + nz, nc)

        @pl.when(i > 0)
        def _():
            cur_copy(last, b, d + (half - 1)).wait_recv()

        out[pl.ds(pl.multiple_of(b * blk, blk), blk), :] = cur[last, b]
        return carry

    lax.fori_loop(0, nc, put_block, 0)

    for layer in range(layers):
        for k in range(1, nc):
            to = lax.rem(c + k, nc)
            part_copy(layer, to, c).wait_send()
            halo_copy(layer, to, c).wait_send()
            hid_copy(layer, c, to).wait_send()
        for slot in range(nc):
            if slot != half - 1:
                win_copy(layer, lax.rem(z + slot - (half - 1) + nz, nc), slot).wait_send()
                cur_copy(layer, mine, slot).wait_send()
        for j in range(1, owners):
            sum_copy(layer, rank, j).wait_send()
    for k in range(1, nc):
        norm_copy(c, lax.rem(c + k, nc)).wait_send()


def on_device(
    tokens,
    norm_gains,
    gate_weight,
    value_weight,
    gate_scale,
    value_scale,
    conv_gate,
    conv_value,
    down_weight,
    down_scale,
):
    nz, nc = lax.axis_size("ra"), lax.axis_size("cb")
    rows, width = tokens.shape
    layers, _, ff = gate_weight.shape
    taps = conv_gate.shape[1]
    ffp = (ff + 3 + 127) // 128 * 128
    blk = rows // nc
    owners = nz // nc
    dims = (layers, nz, nc, width, ff, ffp, blk, taps)
    vmem = pl.BlockSpec(memory_space=pltpu.VMEM)
    hbm = pl.BlockSpec(memory_space=pl.ANY)
    dma = pltpu.SemaphoreType.DMA
    return pl.pallas_call(
        functools.partial(kernel, dims),
        out_shape=jax.ShapeDtypeStruct((rows, width), bf16),
        in_specs=[vmem, vmem, hbm, hbm, vmem, vmem, vmem, vmem, hbm, vmem],
        out_specs=vmem,
        scratch_shapes=[
            pltpu.VMEM((layers, 2, width, ff), f32),
            pltpu.VMEM((layers, ff, width), f32),
            pltpu.VMEM((layers, width, 2 * ffp), bf16),
            pltpu.VMEM((layers, ffp, width), bf16),
            pltpu.VMEM((layers, nc, blk, 2 * ffp), bf16),
            pltpu.VMEM((layers, nc, taps - 1, 2 * ffp), bf16),
            pltpu.VMEM((layers, nc, blk, 2 * ffp), bf16),
            pltpu.VMEM((layers, nc, taps - 1, 2 * ffp), bf16),
            pltpu.VMEM((8 + blk, 2 * ffp), f32),
            pltpu.VMEM((layers, nc, blk, ffp), bf16),
            pltpu.VMEM((layers, nc, blk, width), bf16),
            pltpu.VMEM((layers, nc, blk, width), bf16),
            pltpu.VMEM((layers, owners, blk, width), bf16),
            pltpu.VMEM((layers, nc, blk, width), bf16),
            pltpu.VMEM((nc, blk, 128), bf16),
            dma((layers, 3)),
        ]
        + [dma((layers, nc))] * 8
        + [dma((layers, owners))] * 2
        + [dma((layers, nc))] * 2
        + [dma((nc,))] * 2,
        compiler_params=pltpu.CompilerParams(
            collective_id=0, has_side_effects=True, vmem_limit_bytes=40 * 2**20
        ),
        cost_estimate=pl.CostEstimate(flops=4 * 10**8, bytes_accessed=10**7, transcendentals=0),
    )(
        tokens,
        norm_gains,
        gate_weight,
        value_weight,
        gate_scale,
        value_scale,
        conv_gate,
        conv_value,
        down_weight,
        down_scale,
    )


def solution(mesh):
    in_specs = (
        P("grp", "cb"),
        P(None, "cb"),
        P(None, "cb", "ra"),
        P(None, "cb", "ra"),
        P(None, "ra"),
        P(None, "ra"),
        P(None, None, "ra"),
        P(None, None, "ra"),
        P(None, "ra", "cb"),
        P(None, "cb"),
    )
    out_specs = P("grp", "cb")
    return jax.shard_map(on_device, mesh=mesh, in_specs=in_specs, out_specs=out_specs, check_vma=False)
```

```python
import functools

import jax
import jax.numpy as jnp
from jax import lax
from jax.experimental import pallas as pl
from jax.experimental.pallas import tpu as pltpu
from jax.sharding import PartitionSpec as P

epsilon = 1e-06
residual_weight = 0.5
MESH = pl.DeviceIdType.MESH
f32 = jnp.float32
bf16 = jnp.bfloat16


def in_three(column):
    hi = column.astype(bf16).astype(f32)
    mid = (column - hi).astype(bf16).astype(f32)
    lo = (column - hi - mid).astype(bf16).astype(f32)
    return hi, mid, lo


def with_lanes(tile, at, columns):
    lane = lax.broadcasted_iota(jnp.int32, tile.shape, 1)
    for k, column in enumerate(columns):
        tile = jnp.where(lane == at + k, column, tile)
    return tile


def as_row(column):
    n = column.shape[0]
    at = lax.broadcasted_iota(jnp.int32, (n, 128), 0) == lax.broadcasted_iota(jnp.int32, (n, 128), 1)
    return jnp.sum(jnp.where(at, column, 0.0), axis=0, keepdims=True)


def as_column(row, n, first):
    at = lax.broadcasted_iota(jnp.int32, (n, 128), 0) + first == lax.broadcasted_iota(jnp.int32, (n, 128), 1)
    return jnp.sum(jnp.where(at, row, 0.0), axis=1, keepdims=True)


def kernel(
    dims,
    tok_hbm,
    gains_hbm,
    gate_w,
    value_w,
    gate_scale_hbm,
    value_scale_hbm,
    conv_gate_hbm,
    conv_value_hbm,
    down_w,
    down_scale_hbm,
    out,
    tok,
    gains,
    gate_scale,
    value_scale,
    conv_gate,
    conv_value,
    down_scale,
    raw_in,
    raw_down,
    w_first,
    w_later,
    w_down,
    part,
    part_halo,
    got,
    got_halo,
    pre,
    hid,
    down_part,
    win,
    sums,
    cur,
    squares_row,
    inverse_row,
    small_sem,
    w_sem,
    ps,
    pr,
    qs,
    qr,
    gs,
    gr,
    zs,
    zr,
    ms,
    mr,
    bs,
    br,
    ns,
    nr,
    vs,
    vr,
    greeting,
):
    layers, nz, nc, width, ff, ffp, blk, taps = dims
    owners = nz // nc
    half = nc // 2
    rows = blk // 2
    halo = taps - 1
    model_width = width * nc
    z = lax.axis_index("ra")
    c = lax.axis_index("cb")
    mine = lax.rem(z, nc)
    rank = z // nc

    def along_z(d):
        return {"ra": lax.rem(z + d + 2 * nz, nz), "cb": c}

    def along_c(k):
        return {"ra": z, "cb": lax.rem(c + k, nc)}

    def send(src, dst, ssem, rsem, to):
        return pltpu.make_async_remote_copy(
            src_ref=src, dst_ref=dst, send_sem=ssem, recv_sem=rsem, device_id=to, device_id_type=MESH
        )

    barrier = pltpu.get_barrier_semaphore()
    peers = [along_c(k) for k in range(1, nc)] + [along_z(1), along_z(-1)]
    for to in peers:
        pl.semaphore_signal(barrier, inc=1, device_id=to, device_id_type=MESH)

    def greet(stage):
        for d in (-(2**stage), 2**stage):
            pl.semaphore_signal(greeting.at[stage], inc=1, device_id=along_z(d), device_id_type=MESH)

    def greeted(stage):
        pl.semaphore_wait(greeting.at[stage], 2)

    def weight_loads(layer):
        for k, (src, dst) in enumerate(
            (
                (gate_w, raw_in.at[layer, 0, pl.ds(0, ff)]),
                (value_w, raw_in.at[layer, 1, pl.ds(0, ff)]),
                (down_w, raw_down.at[layer]),
            )
        ):
            yield pltpu.make_async_copy(src.at[layer], dst, w_sem.at[layer, k])

    small = [
        pltpu.make_async_copy(src, dst, small_sem.at[k])
        for k, (src, dst) in enumerate(
            (
                (tok_hbm, tok),
                (gains_hbm, gains),
                (gate_scale_hbm, gate_scale),
                (value_scale_hbm, value_scale),
                (conv_gate_hbm, conv_gate),
                (conv_value_hbm, conv_value),
                (down_scale_hbm, down_scale),
            )
        )
    ]
    weights = [list(weight_loads(layer)) for layer in range(layers)]
    for load in small[:2] + weights[0] + small[2:] + sum(weights[1:], []):
        load.start()

    edge = ff // 128 * 128
    for layer in range(layers):
        for s in range(2):
            raw_in[layer, s, ff:, :] = jnp.zeros((ffp - ff, width), f32)
        w_down[layer, ff:, :] = jnp.zeros((ffp - ff, width), bf16)
        part_halo[layer, 0] = jnp.zeros((halo, 2 * ffp), bf16)
        hid[layer, c, :, edge:] = jnp.zeros((blk, ffp - edge), bf16)

    def take_in(layer):
        for s in range(2):
            weights[layer][s].wait()
            if layer == 0:
                w_first[s * ffp : (s + 1) * ffp, :] = raw_in[0, s].astype(bf16)
            else:
                w_later[layer - 1, :, s * ffp : (s + 1) * ffp] = raw_in[layer, s].T.astype(bf16)

    def take_down(layer):
        weights[layer][2].wait()
        w_down[layer, 0:ff, :] = raw_down[layer].astype(bf16)

    def partials(x, layer):
        scaled = (x * gains[layer : layer + 1, :]).astype(bf16)
        if layer == 0:
            p = lax.dot_general(scaled, w_first[...], (((1,), (1,)), ((), ())), preferred_element_type=f32)
        else:
            p = jnp.dot(scaled, w_later[layer - 1], preferred_element_type=f32)
        squares = in_three(jnp.sum(x * x, axis=1, keepdims=True))
        last = with_lanes(p[:, edge:ffp], ff - edge, squares)
        return jnp.concatenate([p[:, :edge], last, p[:, ffp:]], axis=1)

    def part_copy(layer, b, src):
        return send(part.at[layer, b], got.at[layer, src], ps.at[layer, b], pr.at[layer, src], {"ra": z, "cb": b})

    def halo_copy(layer, b, src):
        return send(
            part_halo.at[layer, b], got_halo.at[layer, src], qs.at[layer, b], qr.at[layer, src], {"ra": z, "cb": b}
        )

    def hid_copy(layer, b, to):
        return send(hid.at[layer, b], hid.at[layer, b], gs.at[layer, to], gr.at[layer, b], {"ra": z, "cb": to})

    def away(p, slot):
        return slot - (half - 1) - p

    def slot_of(p, b):
        return lax.rem(b - z + (half - 1) + p + nz, nc)

    def others(p):
        return sorted((s for s in range(nc) if away(p, s) != 0), key=lambda s: -abs(away(p, s)))

    def win_copy(layer, p, b, slot):
        return send(
            down_part.at[layer, b, p],
            win.at[layer, p, slot],
            zs.at[layer, p, b],
            zr.at[layer, p, slot],
            along_z(away(p, slot)),
        )

    def sum_copy(layer, p, k, j):
        return send(
            sums.at[layer, p, k], sums.at[layer, p, k], ms.at[layer, p, j], mr.at[layer, p, k], along_z(nc * j)
        )

    def cur_copy(layer, p, b, slot):
        return send(
            cur.at[layer, b, p],
            cur.at[layer, b, p],
            bs.at[layer, p, slot],
            br.at[layer, p, slot],
            along_z(-away(p, slot)),
        )

    def squares_copy(src, to):
        return send(squares_row.at[src], squares_row.at[src], ns.at[to], nr.at[src], {"ra": z, "cb": to})

    def inverse_copy(p, b, slot):
        return send(
            inverse_row.at[b, p], inverse_row.at[b, p], vs.at[p, slot], vr.at[p, slot], along_z(-away(p, slot))
        )

    def near_first(i):
        return (2 * lax.rem(i, 2) - 1) * ((i + 1) // 2)

    far_c = sorted(range(1, nc), key=lambda k: -min(k, nc - k))
    far_owner = sorted(range(1, owners), key=lambda j: -min(j, owners - j))

    for layer in range(layers):
        if layer == 0:
            small[0].wait()
            small[1].wait()
            take_in(0)
            p = partials(tok[...].astype(f32), 0).reshape(nc, blk, 2 * ffp)
            part[0] = p.astype(bf16)
            for b in range(1, nc):
                part_halo[0, b] = p[b - 1, blk - halo :, :].astype(bf16)
            pl.semaphore_wait(barrier, len(peers))
            for k in far_c:
                to = lax.rem(c + k, nc)
                part_copy(0, to, c).start()
                halo_copy(0, to, c).start()
            greet(0)
        else:

            def one_block(i, carry, layer=layer):
                b = lax.rem(z + near_first(i) + nz, nc)

                @pl.when(i > 0)
                def _():
                    for p in range(2):
                        cur_copy(layer - 1, p, b, slot_of(p, b)).wait_recv()

                p = partials(cur[layer - 1, b].reshape(blk, width).astype(f32), layer)
                part[layer, b] = p.astype(bf16)

                @pl.when(b != c)
                def _():
                    part_copy(layer, b, c).start()

                after = lax.rem(b + 1, nc)

                @pl.when(after != 0)
                def _():
                    part_halo[layer, after] = p[blk - halo :, :].astype(bf16)

                @pl.when(after != c)
                def _():
                    halo_copy(layer, after, c).start()

                return carry

            lax.fori_loop(0, nc, one_block, 0)

        got[layer, c] = part[layer, c]
        got_halo[layer, c] = part_halo[layer, c]
        if layer == 0:
            take_down(0)
            greeted(0)
            greet(1)
            for load in small[2:]:
                load.wait()
        for k in range(1, nc):
            src = lax.rem(c + k, nc)
            part_copy(layer, c, src).wait_recv()
            halo_copy(layer, c, src).wait_recv()
        for buf, count, at in ((got_halo, halo, 8 - halo), (got, blk, 8)):
            total = buf[layer, 0].astype(f32)
            for src in range(1, nc):
                total = total + buf[layer, src].astype(f32)
            squares = jnp.sum(total[:, ff : ff + 3], axis=1, keepdims=True)
            inverse = lax.rsqrt(squares / model_width + epsilon)
            pre[at : at + count, 0:ff] = inverse * gate_scale[layer : layer + 1, :] * total[:, 0:ff]
            pre[at : at + count, ffp : ffp + ff] = (
                inverse * value_scale[layer : layer + 1, :] * total[:, ffp : ffp + ff]
            )
        convs = []
        for lane, tap_weights in ((0, conv_gate), (ffp, conv_value)):
            y = None
            for k in range(taps):
                term = pre[8 - halo + k : 8 - halo + k + blk, lane : lane + ff] * tap_weights[k, layer : layer + 1, :]
                y = term if y is None else y + term
            convs.append(y)
        hid[layer, c, :, 0:ff] = (jax.nn.gelu(convs[0], approximate=True) * convs[1]).astype(bf16)
        for k in far_c:
            hid_copy(layer, c, lax.rem(c + k, nc)).start()
        if layer == 0:
            greeted(1)
            greet(2)

        def down_block(i, carry, layer=layer):
            b = lax.rem(c + near_first(i) + nc, nc)

            @pl.when(i > 0)
            def _():
                hid_copy(layer, b, c).wait_recv()

            d = jnp.dot(hid[layer, b], w_down[layer], preferred_element_type=f32)
            down_part[layer, b] = d.astype(bf16).reshape(2, rows, width)
            slot = slot_of(0, b)

            @pl.when(slot != half - 1)
            def _():
                win_copy(layer, 0, b, slot).start()

            return carry

        lax.fori_loop(0, nc, down_block, 0)
        for slot in others(1):
            win_copy(layer, 1, lax.rem(z + away(1, slot) + nz, nc), slot).start()
        if layer + 1 < layers:
            take_in(layer + 1)
            take_down(layer + 1)
        if layer == 0:
            greeted(2)
            greet(3)

        for p in range(2):
            win[layer, p, half - 1 + p] = down_part[layer, mine, p]
            for slot in others(p):
                win_copy(layer, p, mine, slot).wait_recv()
            total = win[layer, p, 0].astype(f32)
            for slot in range(1, nc):
                total = total + win[layer, p, slot].astype(f32)
            sums[layer, p, rank] = total.astype(bf16)
            if layer == 0 and p == 0:
                greeted(3)
            for j in far_owner:
                sum_copy(layer, p, rank, j).start()
        lengths = []
        for p in range(2):
            for j in far_owner:
                sum_copy(layer, p, lax.rem(rank + j, owners), j).wait_recv()
            total = sums[layer, p, 0].astype(f32)
            for k in range(1, owners):
                total = total + sums[layer, p, k].astype(f32)
            if layer == 0:
                own = tok[pl.ds(pl.multiple_of(mine * blk + p * rows, rows), rows), :].astype(f32)
            else:
                own = cur[layer - 1, mine, p].astype(f32)
            new = (residual_weight * own + down_scale[layer : layer + 1, :] * total).astype(bf16)
            cur[layer, mine, p] = new
            for slot in others(p):
                cur_copy(layer, p, mine, slot).start()
            if layer == layers - 1:
                wide = new.astype(f32)
                lengths.append(jnp.sum(wide * wide, axis=1, keepdims=True))

    squares_row[c] = as_row(jnp.concatenate(lengths, axis=0))
    for k in far_c:
        squares_copy(c, lax.rem(c + k, nc)).start()
    for k in range(1, nc):
        squares_copy(lax.rem(c + k, nc), c).wait_recv()
    total = squares_row[0]
    for k in range(1, nc):
        total = total + squares_row[k]
    inverse = lax.rsqrt(total / model_width + epsilon)
    for p in range(2):
        inverse_row[mine, p] = inverse
    for p in range(2):
        for slot in others(p):
            inverse_copy(p, mine, slot).start()

    last = layers - 1

    def put_block(i, carry):
        b = lax.rem(z + near_first(i) + nz, nc)

        @pl.when(i > 0)
        def _():
            for p in range(2):
                cur_copy(last, p, b, slot_of(p, b)).wait_recv()
                inverse_copy(p, b, slot_of(p, b)).wait_recv()

        for p in range(2):
            scale = as_column(inverse_row[b, p], rows, p * rows)
            wide = cur[last, b, p].astype(f32) * scale * gains[layers : layers + 1, :]
            out[pl.ds(pl.multiple_of(b * blk + p * rows, rows), rows), :] = wide.astype(bf16)
        return carry

    lax.fori_loop(0, nc, put_block, 0)

    for layer in range(layers):
        for k in range(1, nc):
            to = lax.rem(c + k, nc)
            part_copy(layer, to, c).wait_send()
            halo_copy(layer, to, c).wait_send()
            hid_copy(layer, c, to).wait_send()
        for p in range(2):
            for slot in others(p):
                win_copy(layer, p, lax.rem(z + away(p, slot) + nz, nc), slot).wait_send()
                cur_copy(layer, p, mine, slot).wait_send()
            for j in range(1, owners):
                sum_copy(layer, p, rank, j).wait_send()
    for k in range(1, nc):
        squares_copy(c, lax.rem(c + k, nc)).wait_send()
    for p in range(2):
        for slot in others(p):
            inverse_copy(p, mine, slot).wait_send()


def on_device(
    tokens,
    norm_gains,
    gate_weight,
    value_weight,
    gate_scale,
    value_scale,
    conv_gate,
    conv_value,
    down_weight,
    down_scale,
):
    nz, nc = lax.axis_size("ra"), lax.axis_size("cb")
    rows, width = tokens.shape
    layers, _, ff = gate_weight.shape
    taps = conv_gate.shape[1]
    ffp = (ff + 3 + 127) // 128 * 128
    blk = rows // nc
    owners = nz // nc
    dims = (layers, nz, nc, width, ff, ffp, blk, taps)
    dma = pltpu.SemaphoreType.DMA
    operands = (
        tokens,
        norm_gains,
        gate_weight.swapaxes(1, 2),
        value_weight.swapaxes(1, 2),
        gate_scale,
        value_scale,
        conv_gate.swapaxes(0, 1),
        conv_value.swapaxes(0, 1),
        down_weight,
        down_scale,
    )
    small = [operands[k] for k in (0, 1, 4, 5, 6, 7, 9)]
    return pl.pallas_call(
        functools.partial(kernel, dims),
        out_shape=jax.ShapeDtypeStruct((rows, width), bf16),
        in_specs=[pl.BlockSpec(memory_space=pltpu.HBM)] * len(operands),
        out_specs=pl.BlockSpec(memory_space=pltpu.VMEM),
        scratch_shapes=[pltpu.VMEM(a.shape, a.dtype) for a in small]
        + [
            pltpu.VMEM((layers, 2, ffp, width), f32),
            pltpu.VMEM((layers, ff, width), f32),
            pltpu.VMEM((2 * ffp, width), bf16),
            pltpu.VMEM((layers - 1, width, 2 * ffp), bf16),
            pltpu.VMEM((layers, ffp, width), bf16),
            pltpu.VMEM((layers, nc, blk, 2 * ffp), bf16),
            pltpu.VMEM((layers, nc, taps - 1, 2 * ffp), bf16),
            pltpu.VMEM((layers, nc, blk, 2 * ffp), bf16),
            pltpu.VMEM((layers, nc, taps - 1, 2 * ffp), bf16),
            pltpu.VMEM((8 + blk, 2 * ffp), f32),
            pltpu.VMEM((layers, nc, blk, ffp), bf16),
            pltpu.VMEM((layers, nc, 2, blk // 2, width), bf16),
            pltpu.VMEM((layers, 2, nc, blk // 2, width), bf16),
            pltpu.VMEM((layers, 2, owners, blk // 2, width), bf16),
            pltpu.VMEM((layers, nc, 2, blk // 2, width), bf16),
            pltpu.VMEM((nc, 1, 128), f32),
            pltpu.VMEM((nc, 2, 1, 128), f32),
            dma((len(small),)),
            dma((layers, 3)),
        ]
        + [dma((layers, nc))] * 6
        + [dma((layers, 2, nc))] * 2
        + [dma((layers, 2, owners))] * 2
        + [dma((layers, 2, nc))] * 2
        + [dma((nc,))] * 2
        + [dma((2, nc))] * 2
        + [pltpu.SemaphoreType.REGULAR((4,))],
        compiler_params=pltpu.CompilerParams(
            collective_id=0, has_side_effects=True, vmem_limit_bytes=61 * 2**20
        ),
        cost_estimate=pl.CostEstimate(flops=4 * 10**8, bytes_accessed=10**7, transcendentals=0),
    )(*operands)


def solution(mesh):
    in_specs = (
        P("grp", "cb"),
        P(None, "cb"),
        P(None, "cb", "ra"),
        P(None, "cb", "ra"),
        P(None, "ra"),
        P(None, "ra"),
        P(None, None, "ra"),
        P(None, None, "ra"),
        P(None, "ra", "cb"),
        P(None, "cb"),
    )
    out_specs = P("grp", "cb")
    return jax.shard_map(on_device, mesh=mesh, in_specs=in_specs, out_specs=out_specs, check_vma=False)
```

```python
import functools

import jax
import jax.numpy as jnp
from jax import lax
from jax.experimental import pallas as pl
from jax.experimental.pallas import tpu as pltpu
from jax.sharding import PartitionSpec as P

epsilon = 1e-06
residual_weight = 0.5
MESH = pl.DeviceIdType.MESH
f32 = jnp.float32
bf16 = jnp.bfloat16


def in_three(column):
    hi = column.astype(bf16).astype(f32)
    mid = (column - hi).astype(bf16).astype(f32)
    lo = (column - hi - mid).astype(bf16).astype(f32)
    return hi, mid, lo


def with_lanes(tile, at, columns):
    lane = lax.broadcasted_iota(jnp.int32, tile.shape, 1)
    for k, column in enumerate(columns):
        tile = jnp.where(lane == at + k, column, tile)
    return tile


def as_row(column):
    n = column.shape[0]
    at = lax.broadcasted_iota(jnp.int32, (n, 128), 0) == lax.broadcasted_iota(jnp.int32, (n, 128), 1)
    return jnp.sum(jnp.where(at, column, 0.0), axis=0, keepdims=True)


def as_column(row, n, first):
    at = lax.broadcasted_iota(jnp.int32, (n, 128), 0) + first == lax.broadcasted_iota(jnp.int32, (n, 128), 1)
    return jnp.sum(jnp.where(at, row, 0.0), axis=1, keepdims=True)


def kernel(
    dims,
    tok_hbm,
    gains_hbm,
    gate_w,
    value_w,
    gate_scale_hbm,
    value_scale_hbm,
    conv_gate_hbm,
    conv_value_hbm,
    down_w,
    down_scale_hbm,
    out,
    tok,
    gains,
    gate_scale,
    value_scale,
    conv_gate,
    conv_value,
    down_scale,
    raw_in,
    raw_down,
    w_first,
    w_later,
    w_down,
    part,
    part_halo,
    got,
    got_halo,
    pre,
    hid,
    down_part,
    win,
    sums,
    cur,
    squares_row,
    inverse_row,
    result,
    small_sem,
    w_sem,
    ps,
    pr,
    qs,
    qr,
    gs,
    gr,
    zs,
    zr,
    ms,
    mr,
    bs,
    br,
    ns,
    nr,
    vs,
    vr,
    out_sem,
    greeting,
):
    layers, nz, nc, width, ff, ffp, blk, taps = dims
    owners = nz // nc
    half = nc // 2
    rows = blk // 2
    halo = taps - 1
    model_width = width * nc
    z = lax.axis_index("ra")
    c = lax.axis_index("cb")
    mine = lax.rem(z, nc)
    rank = z // nc

    def along_z(d):
        return {"ra": lax.rem(z + d + 2 * nz, nz), "cb": c}

    def along_c(k):
        return {"ra": z, "cb": lax.rem(c + k, nc)}

    def send(src, dst, ssem, rsem, to):
        return pltpu.make_async_remote_copy(
            src_ref=src, dst_ref=dst, send_sem=ssem, recv_sem=rsem, device_id=to, device_id_type=MESH
        )

    barrier = pltpu.get_barrier_semaphore()
    peers = [along_c(k) for k in range(1, nc)] + [along_z(1), along_z(-1)]
    for to in peers:
        pl.semaphore_signal(barrier, inc=1, device_id=to, device_id_type=MESH)

    def greet(stage):
        for d in (-(2**stage), 2**stage):
            pl.semaphore_signal(greeting.at[stage], inc=1, device_id=along_z(d), device_id_type=MESH)

    def greeted(stage):
        pl.semaphore_wait(greeting.at[stage], 2)

    def weight_loads(layer):
        for k, (src, dst) in enumerate(
            (
                (gate_w, raw_in.at[layer, 0, pl.ds(0, ff)]),
                (value_w, raw_in.at[layer, 1, pl.ds(0, ff)]),
                (down_w, raw_down.at[layer]),
            )
        ):
            yield pltpu.make_async_copy(src.at[layer], dst, w_sem.at[layer, k])

    small = [
        pltpu.make_async_copy(src, dst, small_sem.at[k])
        for k, (src, dst) in enumerate(
            (
                (tok_hbm, tok),
                (gains_hbm, gains),
                (gate_scale_hbm, gate_scale),
                (value_scale_hbm, value_scale),
                (conv_gate_hbm, conv_gate),
                (conv_value_hbm, conv_value),
                (down_scale_hbm, down_scale),
            )
        )
    ]
    weights = [list(weight_loads(layer)) for layer in range(layers)]
    for load in small[:2] + weights[0] + small[2:] + sum(weights[1:], []):
        load.start()

    edge = ff // 128 * 128
    for layer in range(layers):
        for s in range(2):
            raw_in[layer, s, ff:, :] = jnp.zeros((ffp - ff, width), f32)
        w_down[layer, ff:, :] = jnp.zeros((ffp - ff, width), bf16)
        part_halo[layer, 0] = jnp.zeros((halo, 2 * ffp), bf16)
        hid[layer, c, :, edge:] = jnp.zeros((blk, ffp - edge), bf16)

    def take_in(layer):
        for s in range(2):
            weights[layer][s].wait()
            if layer == 0:
                w_first[s * ffp : (s + 1) * ffp, :] = raw_in[0, s].astype(bf16)
            else:
                w_later[layer - 1, :, s * ffp : (s + 1) * ffp] = raw_in[layer, s].T.astype(bf16)

    def take_down(layer):
        weights[layer][2].wait()
        w_down[layer, 0:ff, :] = raw_down[layer].astype(bf16)

    def partials(x, layer):
        scaled = (x * gains[layer : layer + 1, :]).astype(bf16)
        if layer == 0:
            p = lax.dot_general(scaled, w_first[...], (((1,), (1,)), ((), ())), preferred_element_type=f32)
        else:
            p = jnp.dot(scaled, w_later[layer - 1], preferred_element_type=f32)
        squares = in_three(jnp.sum(x * x, axis=1, keepdims=True))
        last = with_lanes(p[:, edge:ffp], ff - edge, squares)
        return jnp.concatenate([p[:, :edge], last, p[:, ffp:]], axis=1)

    most = pl.ds(0, nc - 1)

    def part_copy(layer, b, src):
        return send(part.at[layer, b], got.at[layer, src], ps.at[layer], pr.at[layer], {"ra": z, "cb": b})

    def part_all(layer):
        return send(part.at[layer, most], got.at[layer, most], ps.at[layer], pr.at[layer], along_c(1))

    def halo_copy(layer, b, src):
        return send(part_halo.at[layer, b], got_halo.at[layer, src], qs.at[layer], qr.at[layer], {"ra": z, "cb": b})

    def halo_all(layer):
        return send(part_halo.at[layer, most], got_halo.at[layer, most], qs.at[layer], qr.at[layer], along_c(1))

    def hid_copy(layer, b, to):
        return send(hid.at[layer, b], hid.at[layer, b], gs.at[layer], gr.at[layer, b], {"ra": z, "cb": to})

    def hid_all(layer):
        return send(hid.at[layer, most], hid.at[layer, most], gs.at[layer], gr.at[layer, 0], along_c(1))

    def away(p, slot):
        return slot - (half - 1) - p

    def slot_of(p, b):
        return lax.rem(b - z + (half - 1) + p + nz, nc)

    def others(p):
        return sorted((s for s in range(nc) if away(p, s) != 0), key=lambda s: -abs(away(p, s)))

    def win_copy(layer, p, b, slot):
        return send(
            down_part.at[layer, b, p],
            win.at[layer, p, slot],
            zs.at[layer],
            zr.at[layer, p],
            along_z(away(p, slot)),
        )

    def win_got(layer, p):
        return send(win.at[layer, p, most], win.at[layer, p, most], zs.at[layer], zr.at[layer, p], along_z(1))

    def win_sent(layer):
        return send(down_part.at[layer, most], down_part.at[layer, most], zs.at[layer], zr.at[layer, 0], along_z(1))

    def sum_copy(layer, p, k, j):
        return send(sums.at[layer, p, k], sums.at[layer, p, k], ms.at[layer], mr.at[layer, p], along_z(nc * j))

    def sum_got(layer, p):
        three = sums.at[layer, p, pl.ds(0, owners - 1)]
        return send(three, three, ms.at[layer], mr.at[layer, p], along_z(nc))

    def sum_sent(layer):
        six = sums.at[layer, pl.ds(0, 2), pl.ds(0, owners - 1)]
        return send(six, six, ms.at[layer], mr.at[layer, 0], along_z(nc))

    def cur_copy(layer, p, b, slot):
        return send(
            cur.at[layer, b, p],
            cur.at[layer, b, p],
            bs.at[layer],
            br.at[layer, b],
            along_z(-away(p, slot)),
        )

    def cur_got(layer, b):
        return send(cur.at[layer, b], cur.at[layer, b], bs.at[layer], br.at[layer, b], along_z(1))

    def cur_sent(layer):
        return send(cur.at[layer, most], cur.at[layer, most], bs.at[layer], br.at[layer, 0], along_z(1))

    def squares_copy(src, to):
        return send(squares_row.at[src], squares_row.at[src], ns.at[0], nr.at[0], {"ra": z, "cb": to})

    def squares_all():
        return send(squares_row.at[most], squares_row.at[most], ns.at[0], nr.at[0], along_c(1))

    def inverse_copy(p, b, slot):
        return send(inverse_row.at[b, p], inverse_row.at[b, p], vs.at[0], vr.at[b], along_z(-away(p, slot)))

    def inverse_got(b):
        return send(inverse_row.at[b], inverse_row.at[b], vs.at[0], vr.at[b], along_z(1))

    def inverse_sent():
        return send(inverse_row.at[most], inverse_row.at[most], vs.at[0], vr.at[0], along_z(1))

    def near_first(i):
        return (2 * lax.rem(i, 2) - 1) * ((i + 1) // 2)

    far_c = sorted(range(1, nc), key=lambda k: -min(k, nc - k))
    far_owner = sorted(range(1, owners), key=lambda j: -min(j, owners - j))

    for layer in range(layers):
        if layer == 0:
            small[0].wait()
            small[1].wait()
            take_in(0)
            p = partials(tok[...].astype(f32), 0).reshape(nc, blk, 2 * ffp)
            part[0] = p.astype(bf16)
            for b in range(1, nc):
                part_halo[0, b] = p[b - 1, blk - halo :, :].astype(bf16)
            pl.semaphore_wait(barrier, len(peers))
            greet(0)
            for k in far_c:
                to = lax.rem(c + k, nc)
                part_copy(0, to, c).start()
                halo_copy(0, to, c).start()
        else:

            def one_block(i, carry, layer=layer):
                b = lax.rem(z + near_first(i) + nz, nc)

                @pl.when(i > 0)
                def _():
                    cur_got(layer - 1, b).wait_recv()

                p = partials(cur[layer - 1, b].reshape(blk, width).astype(f32), layer)
                part[layer, b] = p.astype(bf16)

                @pl.when(b != c)
                def _():
                    part_copy(layer, b, c).start()

                after = lax.rem(b + 1, nc)

                @pl.when(after != 0)
                def _():
                    part_halo[layer, after] = p[blk - halo :, :].astype(bf16)

                @pl.when(after != c)
                def _():
                    halo_copy(layer, after, c).start()

                return carry

            lax.fori_loop(0, nc, one_block, 0)

        got[layer, c] = part[layer, c]
        got_halo[layer, c] = part_halo[layer, c]
        if layer == 0:
            take_down(0)
            greeted(0)
            greet(1)
            for load in small[2:]:
                load.wait()
            greeted(1)
            greet(2)
        part_all(layer).wait_recv()
        halo_all(layer).wait_recv()
        for buf, count, at in ((got_halo, halo, 8 - halo), (got, blk, 8)):
            total = buf[layer, 0].astype(f32)
            for src in range(1, nc):
                total = total + buf[layer, src].astype(f32)
            squares = jnp.sum(total[:, ff : ff + 3], axis=1, keepdims=True)
            inverse = lax.rsqrt(squares / model_width + epsilon)
            pre[at : at + count, 0:ff] = inverse * gate_scale[layer : layer + 1, :] * total[:, 0:ff]
            pre[at : at + count, ffp : ffp + ff] = (
                inverse * value_scale[layer : layer + 1, :] * total[:, ffp : ffp + ff]
            )
        convs = []
        for lane, tap_weights in ((0, conv_gate), (ffp, conv_value)):
            y = None
            for k in range(taps):
                term = pre[8 - halo + k : 8 - halo + k + blk, lane : lane + ff] * tap_weights[k, layer : layer + 1, :]
                y = term if y is None else y + term
            convs.append(y)
        hid[layer, c, :, 0:ff] = (jax.nn.gelu(convs[0], approximate=True) * convs[1]).astype(bf16)
        for k in far_c:
            hid_copy(layer, c, lax.rem(c + k, nc)).start()
        if layer == 0:
            greeted(2)
            greet(3)

        def down_block(i, carry, layer=layer):
            b = lax.rem(c + near_first(i) + nc, nc)

            @pl.when(i > 0)
            def _():
                hid_copy(layer, b, c).wait_recv()

            d = jnp.dot(hid[layer, b], w_down[layer], preferred_element_type=f32)
            down_part[layer, b] = d.astype(bf16).reshape(2, rows, width)
            slot = slot_of(0, b)

            @pl.when(slot != half - 1)
            def _():
                win_copy(layer, 0, b, slot).start()

            return carry

        lax.fori_loop(0, nc, down_block, 0)
        for slot in others(1):
            win_copy(layer, 1, lax.rem(z + away(1, slot) + nz, nc), slot).start()
        if layer + 1 < layers:
            take_in(layer + 1)
            take_down(layer + 1)

        for p in range(2):
            win[layer, p, half - 1 + p] = down_part[layer, mine, p]
            win_got(layer, p).wait_recv()
            total = win[layer, p, 0].astype(f32)
            for slot in range(1, nc):
                total = total + win[layer, p, slot].astype(f32)
            sums[layer, p, rank] = total.astype(bf16)
            if layer == 0 and p == 0:
                greeted(3)
            for j in far_owner:
                sum_copy(layer, p, rank, j).start()
        lengths = []
        for p in range(2):
            sum_got(layer, p).wait_recv()
            total = sums[layer, p, 0].astype(f32)
            for k in range(1, owners):
                total = total + sums[layer, p, k].astype(f32)
            if layer == 0:
                own = tok[pl.ds(pl.multiple_of(mine * blk + p * rows, rows), rows), :].astype(f32)
            else:
                own = cur[layer - 1, mine, p].astype(f32)
            new = (residual_weight * own + down_scale[layer : layer + 1, :] * total).astype(bf16)
            cur[layer, mine, p] = new
            for slot in others(p):
                cur_copy(layer, p, mine, slot).start()
            if layer == layers - 1:
                wide = new.astype(f32)
                lengths.append(jnp.sum(wide * wide, axis=1, keepdims=True))

    squares_row[c] = as_row(jnp.concatenate(lengths, axis=0))
    for k in far_c:
        squares_copy(c, lax.rem(c + k, nc)).start()
    squares_all().wait_recv()
    total = squares_row[0]
    for k in range(1, nc):
        total = total + squares_row[k]
    inverse = lax.rsqrt(total / model_width + epsilon)
    for p in range(2):
        inverse_row[mine, p] = inverse
    for p in range(2):
        for slot in others(p):
            inverse_copy(p, mine, slot).start()

    last = layers - 1

    def out_copy(b, p):
        there = pl.ds(pl.multiple_of(b * blk + p * rows, rows), rows)
        return pltpu.make_async_copy(result.at[b, p], out.at[there], out_sem.at[0])

    def put_block(i, carry):
        b = lax.rem(z + near_first(i) + nz, nc)

        @pl.when(i > 0)
        def _():
            cur_got(last, b).wait_recv()
            inverse_got(b).wait_recv()

        for p in range(2):
            scale = as_column(inverse_row[b, p], rows, p * rows)
            wide = cur[last, b, p].astype(f32) * scale * gains[layers : layers + 1, :]
            result[b, p] = wide.astype(bf16)
            out_copy(b, p).start()
        return carry

    lax.fori_loop(0, nc, put_block, 0)

    for layer in range(layers):
        for sent in (part_all, halo_all, hid_all, win_sent, sum_sent, cur_sent):
            sent(layer).wait_send()
    squares_all().wait_send()
    inverse_sent().wait_send()
    pltpu.make_async_copy(out, out, out_sem.at[0]).wait()


def on_device(
    tokens,
    norm_gains,
    gate_weight,
    value_weight,
    gate_scale,
    value_scale,
    conv_gate,
    conv_value,
    down_weight,
    down_scale,
):
    nz, nc = lax.axis_size("ra"), lax.axis_size("cb")
    rows, width = tokens.shape
    layers, _, ff = gate_weight.shape
    taps = conv_gate.shape[1]
    ffp = (ff + 3 + 127) // 128 * 128
    blk = rows // nc
    owners = nz // nc
    dims = (layers, nz, nc, width, ff, ffp, blk, taps)
    dma = pltpu.SemaphoreType.DMA
    operands = (
        tokens,
        norm_gains,
        gate_weight.swapaxes(1, 2),
        value_weight.swapaxes(1, 2),
        gate_scale,
        value_scale,
        conv_gate.swapaxes(0, 1),
        conv_value.swapaxes(0, 1),
        down_weight,
        down_scale,
    )
    small = [operands[k] for k in (0, 1, 4, 5, 6, 7, 9)]
    return pl.pallas_call(
        functools.partial(kernel, dims),
        out_shape=jax.ShapeDtypeStruct((rows, width), bf16),
        in_specs=[pl.BlockSpec(memory_space=pltpu.HBM)] * len(operands),
        out_specs=pl.BlockSpec(memory_space=pltpu.HBM),
        scratch_shapes=[pltpu.VMEM(a.shape, a.dtype) for a in small]
        + [
            pltpu.VMEM((layers, 2, ffp, width), f32),
            pltpu.VMEM((layers, ff, width), f32),
            pltpu.VMEM((2 * ffp, width), bf16),
            pltpu.VMEM((layers - 1, width, 2 * ffp), bf16),
            pltpu.VMEM((layers, ffp, width), bf16),
            pltpu.VMEM((layers, nc, blk, 2 * ffp), bf16),
            pltpu.VMEM((layers, nc, taps - 1, 2 * ffp), bf16),
            pltpu.VMEM((layers, nc, blk, 2 * ffp), bf16),
            pltpu.VMEM((layers, nc, taps - 1, 2 * ffp), bf16),
            pltpu.VMEM((8 + blk, 2 * ffp), f32),
            pltpu.VMEM((layers, nc, blk, ffp), bf16),
            pltpu.VMEM((layers, nc, 2, blk // 2, width), bf16),
            pltpu.VMEM((layers, 2, nc, blk // 2, width), bf16),
            pltpu.VMEM((layers, 2, owners, blk // 2, width), bf16),
            pltpu.VMEM((layers, nc, 2, blk // 2, width), bf16),
            pltpu.VMEM((nc, 1, 128), f32),
            pltpu.VMEM((nc, 2, 1, 128), f32),
            pltpu.VMEM((nc, 2, blk // 2, width), bf16),
            dma((len(small),)),
            dma((layers, 3)),
        ]
        + [dma((layers,))] * 5
        + [dma((layers, nc))]
        + [dma((layers,)), dma((layers, 2))] * 2
        + [dma((layers,)), dma((layers, nc))]
        + [dma((1,))] * 3
        + [dma((nc,)), dma((1,))]
        + [pltpu.SemaphoreType.REGULAR((4,))],
        compiler_params=pltpu.CompilerParams(
            collective_id=0, has_side_effects=True, vmem_limit_bytes=61 * 2**20
        ),
        cost_estimate=pl.CostEstimate(flops=4 * 10**8, bytes_accessed=10**7, transcendentals=0),
    )(*operands)


def solution(mesh):
    in_specs = (
        P("grp", "cb"),
        P(None, "cb"),
        P(None, "cb", "ra"),
        P(None, "cb", "ra"),
        P(None, "ra"),
        P(None, "ra"),
        P(None, None, "ra"),
        P(None, None, "ra"),
        P(None, "ra", "cb"),
        P(None, "cb"),
    )
    out_specs = P("grp", "cb")
    return jax.shard_map(on_device, mesh=mesh, in_specs=in_specs, out_specs=out_specs, check_vma=False)
```

```python
import functools

import jax
import jax.numpy as jnp
from jax import lax
from jax.experimental import pallas as pl
from jax.experimental.pallas import tpu as pltpu
from jax.sharding import PartitionSpec as P

epsilon = 1e-06
residual_weight = 0.5
MESH = pl.DeviceIdType.MESH
f32 = jnp.float32
bf16 = jnp.bfloat16


def in_three(column):
    hi = column.astype(bf16).astype(f32)
    mid = (column - hi).astype(bf16).astype(f32)
    lo = (column - hi - mid).astype(bf16).astype(f32)
    return hi, mid, lo


def with_lanes(tile, at, columns):
    lane = lax.broadcasted_iota(jnp.int32, tile.shape, 1)
    for k, column in enumerate(columns):
        tile = jnp.where(lane == at + k, column, tile)
    return tile


def as_row(column):
    n = column.shape[0]
    at = lax.broadcasted_iota(jnp.int32, (n, 128), 0) == lax.broadcasted_iota(jnp.int32, (n, 128), 1)
    return jnp.sum(jnp.where(at, column, 0.0), axis=0, keepdims=True)


def as_column(row, n):
    at = lax.broadcasted_iota(jnp.int32, (n, 128), 0) == lax.broadcasted_iota(jnp.int32, (n, 128), 1)
    return jnp.sum(jnp.where(at, row, 0.0), axis=1, keepdims=True)


def kernel(
    dims,
    tok_hbm,
    gains_hbm,
    gate_w,
    value_w,
    gate_scale_hbm,
    value_scale_hbm,
    conv_gate_hbm,
    conv_value_hbm,
    down_w,
    down_scale_hbm,
    out,
    tok,
    gains,
    gate_scale,
    value_scale,
    conv_gate,
    conv_value,
    down_scale,
    raw_in,
    raw_down,
    w_first,
    w_later,
    w_down,
    part,
    part_halo,
    got,
    got_halo,
    pre,
    hid,
    down_part,
    win,
    sums,
    cur,
    squares_row,
    inverse_row,
    result,
    small_sem,
    w_sem,
    ps,
    pr,
    qs,
    qr,
    gs,
    gr,
    zs,
    zr,
    ms,
    mr,
    bs,
    br,
    ns,
    nr,
    vs,
    vr,
    out_sem,
    greeting,
):
    layers, nz, nc, width, ff, ffp, blk, taps = dims
    owners = nz // nc
    half = nc // 2
    rows = blk
    halo = taps - 1
    model_width = width * nc
    z = lax.axis_index("ra")
    c = lax.axis_index("cb")
    mine = lax.rem(z, nc)
    rank = z // nc

    def along_z(d):
        return {"ra": lax.rem(z + d + 2 * nz, nz), "cb": c}

    def along_c(k):
        return {"ra": z, "cb": lax.rem(c + k, nc)}

    def send(src, dst, ssem, rsem, to):
        return pltpu.make_async_remote_copy(
            src_ref=src, dst_ref=dst, send_sem=ssem, recv_sem=rsem, device_id=to, device_id_type=MESH
        )

    barrier = pltpu.get_barrier_semaphore()
    peers = [along_c(k) for k in range(1, nc)] + [along_z(1), along_z(-1)]
    for to in peers:
        pl.semaphore_signal(barrier, inc=1, device_id=to, device_id_type=MESH)

    def greet(stage):
        for d in (-(2**stage), 2**stage):
            pl.semaphore_signal(greeting.at[stage], inc=1, device_id=along_z(d), device_id_type=MESH)

    def greeted(stage):
        pl.semaphore_wait(greeting.at[stage], 2)

    def weight_loads(layer):
        for k, (src, dst) in enumerate(
            (
                (gate_w, raw_in.at[layer, 0, pl.ds(0, ff)]),
                (value_w, raw_in.at[layer, 1, pl.ds(0, ff)]),
                (down_w, raw_down.at[layer]),
            )
        ):
            yield pltpu.make_async_copy(src.at[layer], dst, w_sem.at[layer, k])

    small = [
        pltpu.make_async_copy(src, dst, small_sem.at[k])
        for k, (src, dst) in enumerate(
            (
                (tok_hbm, tok),
                (gains_hbm, gains),
                (gate_scale_hbm, gate_scale),
                (value_scale_hbm, value_scale),
                (conv_gate_hbm, conv_gate),
                (conv_value_hbm, conv_value),
                (down_scale_hbm, down_scale),
            )
        )
    ]
    weights = [list(weight_loads(layer)) for layer in range(layers)]
    for load in small[:2] + weights[0] + small[2:] + sum(weights[1:], []):
        load.start()

    edge = ff // 128 * 128
    for layer in range(layers):
        for s in range(2):
            raw_in[layer, s, ff:, :] = jnp.zeros((ffp - ff, width), f32)
        w_down[layer, ff:, :] = jnp.zeros((ffp - ff, width), bf16)
        part_halo[layer, 0, 0] = jnp.zeros((halo, 2 * ffp), bf16)
        for p in range(2):
            hid[layer, p, c, :, edge:] = jnp.zeros((blk, ffp - edge), bf16)

    def take_in(layer):
        for s in range(2):
            weights[layer][s].wait()
            if layer == 0:
                w_first[s * ffp : (s + 1) * ffp, :] = raw_in[0, s].astype(bf16)
            else:
                w_later[layer - 1, :, s * ffp : (s + 1) * ffp] = raw_in[layer, s].T.astype(bf16)

    def take_down(layer):
        weights[layer][2].wait()
        w_down[layer, 0:ff, :] = raw_down[layer].astype(bf16)

    def partials(x, layer):
        scaled = (x * gains[layer : layer + 1, :]).astype(bf16)
        if layer == 0:
            p = lax.dot_general(scaled, w_first[...], (((1,), (1,)), ((), ())), preferred_element_type=f32)
        else:
            p = jnp.dot(scaled, w_later[layer - 1], preferred_element_type=f32)
        squares = in_three(jnp.sum(x * x, axis=1, keepdims=True))
        last = with_lanes(p[:, edge:ffp], ff - edge, squares)
        return jnp.concatenate([p[:, :edge], last, p[:, ffp:]], axis=1)

    most = pl.ds(0, nc - 1)

    def part_copy(layer, p, b):
        return send(part.at[layer, p, b], got.at[layer, p, c], ps.at[layer], pr.at[layer, p], {"ra": z, "cb": b})

    def part_got(layer, p):
        ref = got.at[layer, p, most]
        return send(ref, ref, ps.at[layer], pr.at[layer, p], along_c(1))

    def part_sent(layer):
        ref = part.at[layer, pl.ds(0, 2), most]
        return send(ref, ref, ps.at[layer], pr.at[layer, 0], along_c(1))

    def halo_copy(layer, p, b):
        return send(
            part_halo.at[layer, p, b], got_halo.at[layer, p, c], qs.at[layer], qr.at[layer, p], {"ra": z, "cb": b}
        )

    def halo_got(layer, p):
        ref = got_halo.at[layer, p, most]
        return send(ref, ref, qs.at[layer], qr.at[layer, p], along_c(1))

    def halo_sent(layer):
        ref = part_halo.at[layer, pl.ds(0, 2), most]
        return send(ref, ref, qs.at[layer], qr.at[layer, 0], along_c(1))

    def hid_copy(layer, p, b, to):
        return send(hid.at[layer, p, b], hid.at[layer, p, b], gs.at[layer], gr.at[layer, p, b], {"ra": z, "cb": to})

    def hid_sent(layer):
        ref = hid.at[layer, pl.ds(0, 2), most]
        return send(ref, ref, gs.at[layer], gr.at[layer, 0, 0], along_c(1))

    def away(p, slot):
        return slot - (half - 1) - p

    def slot_of(p, b):
        return lax.rem(b - z + (half - 1) + p + nz, nc)

    def others(p):
        return sorted((s for s in range(nc) if away(p, s) != 0), key=lambda s: -abs(away(p, s)))

    def win_copy(layer, p, b, slot):
        return send(
            down_part.at[layer, p, b],
            win.at[layer, p, slot],
            zs.at[layer],
            zr.at[layer, p],
            along_z(away(p, slot)),
        )

    def win_got(layer, p):
        return send(win.at[layer, p, most], win.at[layer, p, most], zs.at[layer], zr.at[layer, p], along_z(1))

    def win_sent(layer):
        ref = down_part.at[layer, pl.ds(0, 2), most]
        return send(ref, ref, zs.at[layer], zr.at[layer, 0], along_z(1))

    def sum_copy(layer, p, k, j):
        return send(sums.at[layer, p, k], sums.at[layer, p, k], ms.at[layer], mr.at[layer, p], along_z(nc * j))

    def sum_got(layer, p):
        three = sums.at[layer, p, pl.ds(0, owners - 1)]
        return send(three, three, ms.at[layer], mr.at[layer, p], along_z(nc))

    def sum_sent(layer):
        six = sums.at[layer, pl.ds(0, 2), pl.ds(0, owners - 1)]
        return send(six, six, ms.at[layer], mr.at[layer, 0], along_z(nc))

    def cur_copy(layer, p, b, slot):
        ref = cur.at[layer, p, b]
        return send(ref, ref, bs.at[layer], br.at[layer, p, b], along_z(-away(p, slot)))

    def cur_got(layer, p, b):
        ref = cur.at[layer, p, b]
        return send(ref, ref, bs.at[layer], br.at[layer, p, b], along_z(1))

    def cur_sent(layer):
        ref = cur.at[layer, pl.ds(0, 2), most]
        return send(ref, ref, bs.at[layer], br.at[layer, 0, 0], along_z(1))

    def squares_copy(p, to):
        ref = squares_row.at[p, c]
        return send(ref, ref, ns.at[0], nr.at[p], {"ra": z, "cb": to})

    def squares_got(p):
        ref = squares_row.at[p, most]
        return send(ref, ref, ns.at[0], nr.at[p], along_c(1))

    def squares_sent():
        ref = squares_row.at[pl.ds(0, 2), most]
        return send(ref, ref, ns.at[0], nr.at[0], along_c(1))

    def inverse_copy(p, b, slot):
        ref = inverse_row.at[p, b]
        return send(ref, ref, vs.at[0], vr.at[p, b], along_z(-away(p, slot)))

    def inverse_got(p, b):
        ref = inverse_row.at[p, b]
        return send(ref, ref, vs.at[0], vr.at[p, b], along_z(1))

    def inverse_sent():
        ref = inverse_row.at[pl.ds(0, 2), most]
        return send(ref, ref, vs.at[0], vr.at[0, 0], along_z(1))

    def near_first(i):
        return (2 * lax.rem(i, 2) - 1) * ((i + 1) // 2)

    far_c = sorted(range(1, nc), key=lambda k: -min(k, nc - k))
    far_owner = sorted(range(1, owners), key=lambda j: -min(j, owners - j))

    for layer in range(layers):
        if layer == 0:
            small[0].wait()
            small[1].wait()
            take_in(0)
            y = partials(tok[...].astype(f32), 0).reshape(2, nc, blk, 2 * ffp)
            part[0] = y.astype(bf16)
            for p in range(2):
                for b in range(nc):
                    if p + b > 0:
                        before = (p, b - 1) if b > 0 else (p - 1, nc - 1)
                        part_halo[0, p, b] = y[before][blk - halo :, :].astype(bf16)
            pl.semaphore_wait(barrier, len(peers))
            greet(0)
            for p in range(2):
                for k in far_c:
                    to = lax.rem(c + k, nc)
                    part_copy(0, p, to).start()
                    halo_copy(0, p, to).start()
        else:
            for p in range(2):
                if p == 0:

                    @pl.when(c != 0)
                    def _(layer=layer):
                        halo_copy(layer, 0, 0).start()

                def two_blocks(i, carry, layer=layer, p=p):
                    b0 = lax.rem(z + near_first(2 * i) + nz, nc)
                    b1 = lax.rem(z + near_first(2 * i + 1) + nz, nc)

                    @pl.when(i > 0)
                    def _():
                        cur_got(layer - 1, p, b0).wait_recv()

                    cur_got(layer - 1, p, b1).wait_recv()
                    x = jnp.concatenate([cur[layer - 1, p, b0], cur[layer - 1, p, b1]], axis=0)
                    y = partials(x.astype(f32), layer)
                    for b, first in ((b0, 0), (b1, blk)):
                        part[layer, p, b] = y[first : first + blk, :].astype(bf16)

                        @pl.when(b != c)
                        def _(b=b):
                            part_copy(layer, p, b).start()

                        ends = y[first + blk - halo : first + blk, :].astype(bf16)
                        after = lax.rem(b + 1, nc)

                        @pl.when(after != 0)
                        def _(after=after, ends=ends):
                            part_halo[layer, p, after] = ends

                            @pl.when(after != c)
                            def _():
                                halo_copy(layer, p, after).start()

                        if p == 0:

                            @pl.when(after == 0)
                            def _(ends=ends):
                                part_halo[layer, 1, 0] = ends

                                @pl.when(c != 0)
                                def _():
                                    halo_copy(layer, 1, 0).start()

                    return carry

                lax.fori_loop(0, nc // 2, two_blocks, 0)

        if layer == 0:
            take_down(0)
            greeted(0)
            greet(1)
            for load in small[2:]:
                load.wait()
            greeted(1)
            greet(2)
        for p in range(2):
            got[layer, p, c] = part[layer, p, c]
            got_halo[layer, p, c] = part_halo[layer, p, c]
            part_got(layer, p).wait_recv()
            halo_got(layer, p).wait_recv()
            for buf, count, at in ((got_halo, halo, 8 - halo), (got, blk, 8)):
                total = buf[layer, p, 0].astype(f32)
                for src in range(1, nc):
                    total = total + buf[layer, p, src].astype(f32)
                squares = jnp.sum(total[:, ff : ff + 3], axis=1, keepdims=True)
                inverse = lax.rsqrt(squares / model_width + epsilon)
                pre[p, at : at + count, 0:ff] = inverse * gate_scale[layer : layer + 1, :] * total[:, 0:ff]
                pre[p, at : at + count, ffp : ffp + ff] = (
                    inverse * value_scale[layer : layer + 1, :] * total[:, ffp : ffp + ff]
                )
            convs = []
            for lane, tap_weights in ((0, conv_gate), (ffp, conv_value)):
                y = None
                for k in range(taps):
                    at = 8 - halo + k
                    term = pre[p, at : at + blk, lane : lane + ff] * tap_weights[k, layer : layer + 1, :]
                    y = term if y is None else y + term
                convs.append(y)
            hid[layer, p, c, :, 0:ff] = (jax.nn.gelu(convs[0], approximate=True) * convs[1]).astype(bf16)
            for k in far_c:
                hid_copy(layer, p, c, lax.rem(c + k, nc)).start()
        if layer == 0:
            greeted(2)
            greet(3)

        for p in range(2):

            def two_downs(i, carry, layer=layer, p=p):
                b0 = lax.rem(c + near_first(2 * i) + nc, nc)
                b1 = lax.rem(c + near_first(2 * i + 1) + nc, nc)

                @pl.when(i > 0)
                def _():
                    hid_copy(layer, p, b0, c).wait_recv()

                hid_copy(layer, p, b1, c).wait_recv()
                h = jnp.concatenate([hid[layer, p, b0], hid[layer, p, b1]], axis=0)
                d = jnp.dot(h, w_down[layer], preferred_element_type=f32).astype(bf16)
                for b, first in ((b0, 0), (b1, blk)):
                    down_part[layer, p, b] = d[first : first + blk, :]
                    slot = slot_of(p, b)

                    @pl.when(slot != half - 1 + p)
                    def _(b=b, slot=slot):
                        win_copy(layer, p, b, slot).start()

                return carry

            lax.fori_loop(0, nc // 2, two_downs, 0)
        if layer + 1 < layers:
            take_in(layer + 1)
            take_down(layer + 1)

        for p in range(2):
            win[layer, p, half - 1 + p] = down_part[layer, p, mine]
            win_got(layer, p).wait_recv()
            total = win[layer, p, 0].astype(f32)
            for slot in range(1, nc):
                total = total + win[layer, p, slot].astype(f32)
            sums[layer, p, rank] = total.astype(bf16)
            if layer == 0 and p == 0:
                greeted(3)
            for j in far_owner:
                sum_copy(layer, p, rank, j).start()
        for p in range(2):
            sum_got(layer, p).wait_recv()
            total = sums[layer, p, 0].astype(f32)
            for k in range(1, owners):
                total = total + sums[layer, p, k].astype(f32)
            if layer == 0:
                own = tok[pl.ds(pl.multiple_of((p * nc + mine) * blk, blk), blk), :].astype(f32)
            else:
                own = cur[layer - 1, p, mine].astype(f32)
            new = (residual_weight * own + down_scale[layer : layer + 1, :] * total).astype(bf16)
            cur[layer, p, mine] = new
            for slot in others(p):
                cur_copy(layer, p, mine, slot).start()
            if layer == layers - 1:
                wide = new.astype(f32)
                squares_row[p, c] = as_row(jnp.sum(wide * wide, axis=1, keepdims=True))
                for k in far_c:
                    squares_copy(p, lax.rem(c + k, nc)).start()

    for p in range(2):
        squares_got(p).wait_recv()
        total = squares_row[p, 0]
        for k in range(1, nc):
            total = total + squares_row[p, k]
        inverse_row[p, mine] = lax.rsqrt(total / model_width + epsilon)
        for slot in others(p):
            inverse_copy(p, mine, slot).start()

    last = layers - 1

    def out_copy(p, b):
        there = pl.ds(pl.multiple_of((p * nc + b) * blk, blk), blk)
        return pltpu.make_async_copy(result.at[p, b], out.at[there], out_sem.at[0])

    for p in range(2):

        def put_block(i, carry, p=p):
            b = lax.rem(z + near_first(i) + nz, nc)

            @pl.when(i > 0)
            def _():
                cur_got(last, p, b).wait_recv()
                inverse_got(p, b).wait_recv()

            scale = as_column(inverse_row[p, b], blk)
            wide = cur[last, p, b].astype(f32) * scale * gains[layers : layers + 1, :]
            result[p, b] = wide.astype(bf16)
            out_copy(p, b).start()
            return carry

        lax.fori_loop(0, nc, put_block, 0)

    for layer in range(layers):
        for sent in (part_sent, halo_sent, hid_sent, win_sent, sum_sent, cur_sent):
            sent(layer).wait_send()
    squares_sent().wait_send()
    inverse_sent().wait_send()
    pltpu.make_async_copy(out, out, out_sem.at[0]).wait()


def on_device(
    tokens,
    norm_gains,
    gate_weight,
    value_weight,
    gate_scale,
    value_scale,
    conv_gate,
    conv_value,
    down_weight,
    down_scale,
):
    nz, nc = lax.axis_size("ra"), lax.axis_size("cb")
    rows, width = tokens.shape
    layers, _, ff = gate_weight.shape
    taps = conv_gate.shape[1]
    ffp = (ff + 3 + 127) // 128 * 128
    blk = rows // (2 * nc)
    owners = nz // nc
    dims = (layers, nz, nc, width, ff, ffp, blk, taps)
    dma = pltpu.SemaphoreType.DMA
    operands = (
        tokens,
        norm_gains,
        gate_weight.swapaxes(1, 2),
        value_weight.swapaxes(1, 2),
        gate_scale,
        value_scale,
        conv_gate.swapaxes(0, 1),
        conv_value.swapaxes(0, 1),
        down_weight,
        down_scale,
    )
    small = [operands[k] for k in (0, 1, 4, 5, 6, 7, 9)]
    return pl.pallas_call(
        functools.partial(kernel, dims),
        out_shape=jax.ShapeDtypeStruct((rows, width), bf16),
        in_specs=[pl.BlockSpec(memory_space=pltpu.HBM)] * len(operands),
        out_specs=pl.BlockSpec(memory_space=pltpu.HBM),
        scratch_shapes=[pltpu.VMEM(a.shape, a.dtype) for a in small]
        + [
            pltpu.VMEM((layers, 2, ffp, width), f32),
            pltpu.VMEM((layers, ff, width), f32),
            pltpu.VMEM((2 * ffp, width), bf16),
            pltpu.VMEM((layers - 1, width, 2 * ffp), bf16),
            pltpu.VMEM((layers, ffp, width), bf16),
            pltpu.VMEM((layers, 2, nc, blk, 2 * ffp), bf16),
            pltpu.VMEM((layers, 2, nc, taps - 1, 2 * ffp), bf16),
            pltpu.VMEM((layers, 2, nc, blk, 2 * ffp), bf16),
            pltpu.VMEM((layers, 2, nc, taps - 1, 2 * ffp), bf16),
            pltpu.VMEM((2, 8 + blk, 2 * ffp), f32),
            pltpu.VMEM((layers, 2, nc, blk, ffp), bf16),
            pltpu.VMEM((layers, 2, nc, blk, width), bf16),
            pltpu.VMEM((layers, 2, nc, blk, width), bf16),
            pltpu.VMEM((layers, 2, owners, blk, width), bf16),
            pltpu.VMEM((layers, 2, nc, blk, width), bf16),
            pltpu.VMEM((2, nc, 1, 128), f32),
            pltpu.VMEM((2, nc, 1, 128), f32),
            pltpu.VMEM((2, nc, blk, width), bf16),
            dma((len(small),)),
            dma((layers, 3)),
        ]
        + [dma((layers,)), dma((layers, 2))] * 2
        + [dma((layers,)), dma((layers, 2, nc))]
        + [dma((layers,)), dma((layers, 2))] * 2
        + [dma((layers,)), dma((layers, 2, nc))]
        + [dma((1,)), dma((2,)), dma((1,)), dma((2, nc)), dma((1,))]
        + [pltpu.SemaphoreType.REGULAR((4,))],
        compiler_params=pltpu.CompilerParams(
            collective_id=0, has_side_effects=True, vmem_limit_bytes=61 * 2**20
        ),
        cost_estimate=pl.CostEstimate(flops=4 * 10**8, bytes_accessed=10**7, transcendentals=0),
    )(*operands)


def solution(mesh):
    in_specs = (
        P("grp", "cb"),
        P(None, "cb"),
        P(None, "cb", "ra"),
        P(None, "cb", "ra"),
        P(None, "ra"),
        P(None, "ra"),
        P(None, None, "ra"),
        P(None, None, "ra"),
        P(None, "ra", "cb"),
        P(None, "cb"),
    )
    out_specs = P("grp", "cb")
    return jax.shard_map(on_device, mesh=mesh, in_specs=in_specs, out_specs=out_specs, check_vma=False)
```

```python
import functools

import jax
import jax.numpy as jnp
from jax import lax
from jax.experimental import pallas as pl
from jax.experimental.pallas import tpu as pltpu
from jax.sharding import PartitionSpec as P

epsilon = 1e-06
residual_weight = 0.5
MESH = pl.DeviceIdType.MESH
f32 = jnp.float32
bf16 = jnp.bfloat16


def in_three(column):
    hi = column.astype(bf16).astype(f32)
    mid = (column - hi).astype(bf16).astype(f32)
    lo = (column - hi - mid).astype(bf16).astype(f32)
    return hi, mid, lo


def with_lanes(tile, at, columns):
    lane = lax.broadcasted_iota(jnp.int32, tile.shape, 1)
    for k, column in enumerate(columns):
        tile = jnp.where(lane == at + k, column, tile)
    return tile


def as_row(column):
    n = column.shape[0]
    at = lax.broadcasted_iota(jnp.int32, (n, 128), 0) == lax.broadcasted_iota(jnp.int32, (n, 128), 1)
    return jnp.sum(jnp.where(at, column, 0.0), axis=0, keepdims=True)


def as_column(row, n):
    at = lax.broadcasted_iota(jnp.int32, (n, 128), 0) == lax.broadcasted_iota(jnp.int32, (n, 128), 1)
    return jnp.sum(jnp.where(at, row, 0.0), axis=1, keepdims=True)


def kernel(
    dims,
    tok_hbm,
    gains_hbm,
    gate_w,
    value_w,
    gate_scale_hbm,
    value_scale_hbm,
    conv_gate_hbm,
    conv_value_hbm,
    down_w,
    down_scale_hbm,
    out,
    tok,
    gains,
    gate_scale,
    value_scale,
    conv_gate,
    conv_value,
    down_scale,
    raw_in,
    raw_down,
    w_first,
    w_later,
    w_down,
    part,
    part_halo,
    got,
    got_halo,
    pre,
    hid,
    down_part,
    win,
    sums,
    cur,
    squares_row,
    inverse_row,
    result,
    small_sem,
    w_sem,
    ps,
    pr,
    qs,
    qr,
    gs,
    gr,
    zs,
    zr,
    ms,
    mr,
    bs,
    br,
    ns,
    nr,
    vs,
    vr,
    out_sem,
    greeting,
):
    layers, nz, nc, width, ff, ffp, blk, taps = dims
    owners = nz // nc
    half = nc // 2
    rows = blk
    halo = taps - 1
    model_width = width * nc
    z = lax.axis_index("ra")
    c = lax.axis_index("cb")
    mine = lax.rem(z, nc)
    rank = z // nc

    def along_z(d):
        return {"ra": lax.rem(z + d + 2 * nz, nz), "cb": c}

    def along_c(k):
        return {"ra": z, "cb": lax.rem(c + k, nc)}

    def send(src, dst, ssem, rsem, to):
        return pltpu.make_async_remote_copy(
            src_ref=src, dst_ref=dst, send_sem=ssem, recv_sem=rsem, device_id=to, device_id_type=MESH
        )

    barrier = pltpu.get_barrier_semaphore()
    peers = [along_c(k) for k in range(1, nc)] + [along_z(1), along_z(-1)]
    for to in peers:
        pl.semaphore_signal(barrier, inc=1, device_id=to, device_id_type=MESH)

    def greet(stage):
        for d in (-(2**stage), 2**stage):
            pl.semaphore_signal(greeting.at[stage], inc=1, device_id=along_z(d), device_id_type=MESH)

    def greeted(stage):
        pl.semaphore_wait(greeting.at[stage], 2)

    def weight_loads(layer):
        for k, (src, dst) in enumerate(
            (
                (gate_w, raw_in.at[layer, 0, pl.ds(0, ff)]),
                (value_w, raw_in.at[layer, 1, pl.ds(0, ff)]),
                (down_w, raw_down.at[layer]),
            )
        ):
            yield pltpu.make_async_copy(src.at[layer], dst, w_sem.at[layer, k])

    small = [
        pltpu.make_async_copy(src, dst, small_sem.at[k])
        for k, (src, dst) in enumerate(
            (
                (tok_hbm, tok),
                (gains_hbm, gains),
                (gate_scale_hbm, gate_scale),
                (value_scale_hbm, value_scale),
                (conv_gate_hbm, conv_gate),
                (conv_value_hbm, conv_value),
                (down_scale_hbm, down_scale),
            )
        )
    ]
    weights = [list(weight_loads(layer)) for layer in range(layers)]
    for load in small[:2] + weights[0] + small[2:] + sum(weights[1:], []):
        load.start()

    edge = ff // 128 * 128
    for layer in range(layers):
        for s in range(2):
            raw_in[layer, s, ff:, :] = jnp.zeros((ffp - ff, width), f32)
        w_down[layer, ff:, :] = jnp.zeros((ffp - ff, width), bf16)
        part_halo[layer, 0, 0] = jnp.zeros((halo, 2 * ffp), bf16)
        for p in range(2):
            hid[layer, p, c, :, edge:] = jnp.zeros((blk, ffp - edge), bf16)

    def take_in(layer):
        for s in range(2):
            weights[layer][s].wait()
            if layer == 0:
                w_first[s * ffp : (s + 1) * ffp, :] = raw_in[0, s].astype(bf16)
            else:
                w_later[layer - 1, :, s * ffp : (s + 1) * ffp] = raw_in[layer, s].T.astype(bf16)

    def take_down(layer):
        weights[layer][2].wait()
        w_down[layer, 0:ff, :] = raw_down[layer].astype(bf16)

    def partials(x, layer):
        scaled = (x * gains[layer : layer + 1, :]).astype(bf16)
        if layer == 0:
            p = lax.dot_general(scaled, w_first[...], (((1,), (1,)), ((), ())), preferred_element_type=f32)
        else:
            p = jnp.dot(scaled, w_later[layer - 1], preferred_element_type=f32)
        squares = in_three(jnp.sum(x * x, axis=1, keepdims=True))
        last = with_lanes(p[:, edge:ffp], ff - edge, squares)
        return jnp.concatenate([p[:, :edge], last, p[:, ffp:]], axis=1)

    most = pl.ds(0, nc - 1)

    def part_copy(layer, p, b):
        return send(part.at[layer, p, b], got.at[layer, p, c], ps.at[layer], pr.at[layer, p], {"ra": z, "cb": b})

    def part_got(layer, p):
        ref = got.at[layer, p, most]
        return send(ref, ref, ps.at[layer], pr.at[layer, p], along_c(1))

    def part_sent(layer):
        ref = part.at[layer, pl.ds(0, 2), most]
        return send(ref, ref, ps.at[layer], pr.at[layer, 0], along_c(1))

    def halo_copy(layer, p, b):
        return send(
            part_halo.at[layer, p, b], got_halo.at[layer, p, c], qs.at[layer], qr.at[layer, p], {"ra": z, "cb": b}
        )

    def halo_got(layer, p):
        ref = got_halo.at[layer, p, most]
        return send(ref, ref, qs.at[layer], qr.at[layer, p], along_c(1))

    def halo_sent(layer):
        ref = part_halo.at[layer, pl.ds(0, 2), most]
        return send(ref, ref, qs.at[layer], qr.at[layer, 0], along_c(1))

    def hid_copy(layer, p, b, to):
        return send(hid.at[layer, p, b], hid.at[layer, p, b], gs.at[layer], gr.at[layer, p, b], {"ra": z, "cb": to})

    def hid_sent(layer):
        ref = hid.at[layer, pl.ds(0, 2), most]
        return send(ref, ref, gs.at[layer], gr.at[layer, 0, 0], along_c(1))

    def away(p, slot):
        return slot - (half - 1) - p

    def slot_of(p, b):
        return lax.rem(b - z + (half - 1) + p + nz, nc)

    def others(p):
        return sorted((s for s in range(nc) if away(p, s) != 0), key=lambda s: -abs(away(p, s)))

    def win_copy(layer, p, b, slot):
        return send(
            down_part.at[layer, p, b],
            win.at[layer, p, slot],
            zs.at[layer],
            zr.at[layer, p],
            along_z(away(p, slot)),
        )

    def win_got(layer, p):
        return send(win.at[layer, p, most], win.at[layer, p, most], zs.at[layer], zr.at[layer, p], along_z(1))

    def win_sent(layer):
        ref = down_part.at[layer, pl.ds(0, 2), most]
        return send(ref, ref, zs.at[layer], zr.at[layer, 0], along_z(1))

    upward = nc * (1 - 2 * lax.rem(rank, 2))

    def sum_copies(layer, p, turn):
        for h, sign in enumerate((1, -1) if turn == 0 else (-1, 1)):
            columns = pl.ds(h * (width // 2), width // 2)
            yield send(
                sums.at[layer, p, 2 * turn, :, columns],
                sums.at[layer, p, 2 * turn + 1, :, columns],
                ms.at[layer],
                mr.at[layer, p, turn],
                along_z(sign * upward),
            )

    def sum_got(layer, p, turn):
        ref = sums.at[layer, p, 2 * turn + 1]
        return send(ref, ref, ms.at[layer], mr.at[layer, p, turn], along_z(nc))

    def sum_sent(layer):
        ref = sums.at[layer, pl.ds(0, 2), pl.ds(0, 2)]
        return send(ref, ref, ms.at[layer], mr.at[layer, 0, 0], along_z(nc))

    def cur_copy(layer, p, b, slot):
        ref = cur.at[layer, p, b]
        return send(ref, ref, bs.at[layer], br.at[layer, p, b], along_z(-away(p, slot)))

    def cur_got(layer, p, b):
        ref = cur.at[layer, p, b]
        return send(ref, ref, bs.at[layer], br.at[layer, p, b], along_z(1))

    def cur_sent(layer):
        ref = cur.at[layer, pl.ds(0, 2), most]
        return send(ref, ref, bs.at[layer], br.at[layer, 0, 0], along_z(1))

    def squares_copy(p, to):
        ref = squares_row.at[p, c]
        return send(ref, ref, ns.at[0], nr.at[p], {"ra": z, "cb": to})

    def squares_got(p):
        ref = squares_row.at[p, most]
        return send(ref, ref, ns.at[0], nr.at[p], along_c(1))

    def squares_sent():
        ref = squares_row.at[pl.ds(0, 2), most]
        return send(ref, ref, ns.at[0], nr.at[0], along_c(1))

    def inverse_copy(p, b, slot):
        ref = inverse_row.at[p, b]
        return send(ref, ref, vs.at[0], vr.at[p, b], along_z(-away(p, slot)))

    def inverse_got(p, b):
        ref = inverse_row.at[p, b]
        return send(ref, ref, vs.at[0], vr.at[p, b], along_z(1))

    def inverse_sent():
        ref = inverse_row.at[pl.ds(0, 2), most]
        return send(ref, ref, vs.at[0], vr.at[0, 0], along_z(1))

    def near_first(i):
        return (2 * lax.rem(i, 2) - 1) * ((i + 1) // 2)

    far_c = sorted(range(1, nc), key=lambda k: -min(k, nc - k))

    def finish(layer, p, total):
        if layer == 0:
            own = tok[pl.ds(pl.multiple_of((p * nc + mine) * blk, blk), blk), :].astype(f32)
        else:
            own = cur[layer - 1, p, mine].astype(f32)
        new = (residual_weight * own + down_scale[layer : layer + 1, :] * total).astype(bf16)
        cur[layer, p, mine] = new
        for slot in others(p):
            cur_copy(layer, p, mine, slot).start()
        if layer == layers - 1:
            wide = new.astype(f32)
            squares_row[p, c] = as_row(jnp.sum(wide * wide, axis=1, keepdims=True))
            for k in far_c:
                squares_copy(p, lax.rem(c + k, nc)).start()

    for layer in range(layers):
        if layer == 0:
            small[0].wait()
            small[1].wait()
            take_in(0)
            y = partials(tok[...].astype(f32), 0).reshape(2, nc, blk, 2 * ffp)
            part[0] = y.astype(bf16)
            for p in range(2):
                for b in range(nc):
                    if p + b > 0:
                        before = (p, b - 1) if b > 0 else (p - 1, nc - 1)
                        part_halo[0, p, b] = y[before][blk - halo :, :].astype(bf16)
            pl.semaphore_wait(barrier, len(peers))
            greet(0)
            for p in range(2):
                for k in far_c:
                    to = lax.rem(c + k, nc)
                    part_copy(0, p, to).start()
                    halo_copy(0, p, to).start()
        else:
            for p in range(2):
                if p == 0:

                    @pl.when(c != 0)
                    def _(layer=layer):
                        halo_copy(layer, 0, 0).start()

                def two_blocks(i, carry, layer=layer, p=p):
                    b0 = lax.rem(z + near_first(2 * i) + nz, nc)
                    b1 = lax.rem(z + near_first(2 * i + 1) + nz, nc)

                    @pl.when(i > 0)
                    def _():
                        cur_got(layer - 1, p, b0).wait_recv()

                    cur_got(layer - 1, p, b1).wait_recv()
                    x = jnp.concatenate([cur[layer - 1, p, b0], cur[layer - 1, p, b1]], axis=0)
                    y = partials(x.astype(f32), layer)
                    for b, first in ((b0, 0), (b1, blk)):
                        part[layer, p, b] = y[first : first + blk, :].astype(bf16)

                        @pl.when(b != c)
                        def _(b=b):
                            part_copy(layer, p, b).start()

                        ends = y[first + blk - halo : first + blk, :].astype(bf16)
                        after = lax.rem(b + 1, nc)

                        @pl.when(after != 0)
                        def _(after=after, ends=ends):
                            part_halo[layer, p, after] = ends

                            @pl.when(after != c)
                            def _():
                                halo_copy(layer, p, after).start()

                        if p == 0:

                            @pl.when(after == 0)
                            def _(ends=ends):
                                part_halo[layer, 1, 0] = ends

                                @pl.when(c != 0)
                                def _():
                                    halo_copy(layer, 1, 0).start()

                    return carry

                lax.fori_loop(0, nc // 2, two_blocks, 0)

        if layer == 0:
            take_down(0)
            greeted(0)
            greet(1)
            for load in small[2:]:
                load.wait()
            greeted(1)
            greet(2)
        for p in range(2):
            got[layer, p, c] = part[layer, p, c]
            got_halo[layer, p, c] = part_halo[layer, p, c]
            part_got(layer, p).wait_recv()
            halo_got(layer, p).wait_recv()
            for buf, count, at in ((got_halo, halo, 8 - halo), (got, blk, 8)):
                total = buf[layer, p, 0].astype(f32)
                for src in range(1, nc):
                    total = total + buf[layer, p, src].astype(f32)
                squares = jnp.sum(total[:, ff : ff + 3], axis=1, keepdims=True)
                inverse = lax.rsqrt(squares / model_width + epsilon)
                pre[p, at : at + count, 0:ff] = inverse * gate_scale[layer : layer + 1, :] * total[:, 0:ff]
                pre[p, at : at + count, ffp : ffp + ff] = (
                    inverse * value_scale[layer : layer + 1, :] * total[:, ffp : ffp + ff]
                )
            convs = []
            for lane, tap_weights in ((0, conv_gate), (ffp, conv_value)):
                y = None
                for k in range(taps):
                    at = 8 - halo + k
                    term = pre[p, at : at + blk, lane : lane + ff] * tap_weights[k, layer : layer + 1, :]
                    y = term if y is None else y + term
                convs.append(y)
            hid[layer, p, c, :, 0:ff] = (jax.nn.gelu(convs[0], approximate=True) * convs[1]).astype(bf16)
            for k in far_c:
                hid_copy(layer, p, c, lax.rem(c + k, nc)).start()

        for p in range(2):

            def two_downs(i, carry, layer=layer, p=p):
                b0 = lax.rem(c + near_first(2 * i) + nc, nc)
                b1 = lax.rem(c + near_first(2 * i + 1) + nc, nc)

                @pl.when(i > 0)
                def _():
                    hid_copy(layer, p, b0, c).wait_recv()

                hid_copy(layer, p, b1, c).wait_recv()
                h = jnp.concatenate([hid[layer, p, b0], hid[layer, p, b1]], axis=0)
                d = jnp.dot(h, w_down[layer], preferred_element_type=f32).astype(bf16)
                for b, first in ((b0, 0), (b1, blk)):
                    down_part[layer, p, b] = d[first : first + blk, :]
                    slot = slot_of(p, b)

                    @pl.when(slot != half - 1 + p)
                    def _(b=b, slot=slot):
                        win_copy(layer, p, b, slot).start()

                return carry

            lax.fori_loop(0, nc // 2, two_downs, 0)
        if layer + 1 < layers:
            take_in(layer + 1)
            take_down(layer + 1)

        for p in range(2):
            win[layer, p, half - 1 + p] = down_part[layer, p, mine]
            win_got(layer, p).wait_recv()
            total = win[layer, p, 0].astype(f32)
            for slot in range(1, nc):
                total = total + win[layer, p, slot].astype(f32)
            sums[layer, p, 0] = total.astype(bf16)
            if layer == 0 and p == 0:
                greeted(2)
            for copy in sum_copies(layer, p, 0):
                copy.start()
        for turn in range(2):
            for p in range(2):
                sum_got(layer, p, turn).wait_recv()
                both = sums[layer, p, 2 * turn].astype(f32) + sums[layer, p, 2 * turn + 1].astype(f32)
                if turn == 0:
                    sums[layer, p, 2] = both.astype(bf16)
                    for copy in sum_copies(layer, p, 1):
                        copy.start()
                else:
                    finish(layer, p, both)

    for p in range(2):
        squares_got(p).wait_recv()
        total = squares_row[p, 0]
        for k in range(1, nc):
            total = total + squares_row[p, k]
        inverse_row[p, mine] = lax.rsqrt(total / model_width + epsilon)
        for slot in others(p):
            inverse_copy(p, mine, slot).start()

    last = layers - 1

    def out_copy(p, b):
        there = pl.ds(pl.multiple_of((p * nc + b) * blk, blk), blk)
        return pltpu.make_async_copy(result.at[p, b], out.at[there], out_sem.at[0])

    for p in range(2):

        def put_block(i, carry, p=p):
            b = lax.rem(z + near_first(i) + nz, nc)

            @pl.when(i > 0)
            def _():
                cur_got(last, p, b).wait_recv()
                inverse_got(p, b).wait_recv()

            scale = as_column(inverse_row[p, b], blk)
            wide = cur[last, p, b].astype(f32) * scale * gains[layers : layers + 1, :]
            result[p, b] = wide.astype(bf16)
            out_copy(p, b).start()
            return carry

        lax.fori_loop(0, nc, put_block, 0)

    for layer in range(layers):
        for sent in (part_sent, halo_sent, hid_sent, win_sent, sum_sent, cur_sent):
            sent(layer).wait_send()
    squares_sent().wait_send()
    inverse_sent().wait_send()
    pltpu.make_async_copy(out, out, out_sem.at[0]).wait()


def on_device(
    tokens,
    norm_gains,
    gate_weight,
    value_weight,
    gate_scale,
    value_scale,
    conv_gate,
    conv_value,
    down_weight,
    down_scale,
):
    nz, nc = lax.axis_size("ra"), lax.axis_size("cb")
    rows, width = tokens.shape
    layers, _, ff = gate_weight.shape
    taps = conv_gate.shape[1]
    ffp = (ff + 3 + 127) // 128 * 128
    blk = rows // (2 * nc)
    owners = nz // nc
    dims = (layers, nz, nc, width, ff, ffp, blk, taps)
    dma = pltpu.SemaphoreType.DMA
    operands = (
        tokens,
        norm_gains,
        gate_weight.swapaxes(1, 2),
        value_weight.swapaxes(1, 2),
        gate_scale,
        value_scale,
        conv_gate.swapaxes(0, 1),
        conv_value.swapaxes(0, 1),
        down_weight,
        down_scale,
    )
    small = [operands[k] for k in (0, 1, 4, 5, 6, 7, 9)]
    return pl.pallas_call(
        functools.partial(kernel, dims),
        out_shape=jax.ShapeDtypeStruct((rows, width), bf16),
        in_specs=[pl.BlockSpec(memory_space=pltpu.HBM)] * len(operands),
        out_specs=pl.BlockSpec(memory_space=pltpu.HBM),
        scratch_shapes=[pltpu.VMEM(a.shape, a.dtype) for a in small]
        + [
            pltpu.VMEM((layers, 2, ffp, width), f32),
            pltpu.VMEM((layers, ff, width), f32),
            pltpu.VMEM((2 * ffp, width), bf16),
            pltpu.VMEM((layers - 1, width, 2 * ffp), bf16),
            pltpu.VMEM((layers, ffp, width), bf16),
            pltpu.VMEM((layers, 2, nc, blk, 2 * ffp), bf16),
            pltpu.VMEM((layers, 2, nc, taps - 1, 2 * ffp), bf16),
            pltpu.VMEM((layers, 2, nc, blk, 2 * ffp), bf16),
            pltpu.VMEM((layers, 2, nc, taps - 1, 2 * ffp), bf16),
            pltpu.VMEM((2, 8 + blk, 2 * ffp), f32),
            pltpu.VMEM((layers, 2, nc, blk, ffp), bf16),
            pltpu.VMEM((layers, 2, nc, blk, width), bf16),
            pltpu.VMEM((layers, 2, nc, blk, width), bf16),
            pltpu.VMEM((layers, 2, owners, blk, width), bf16),
            pltpu.VMEM((layers, 2, nc, blk, width), bf16),
            pltpu.VMEM((2, nc, 1, 128), f32),
            pltpu.VMEM((2, nc, 1, 128), f32),
            pltpu.VMEM((2, nc, blk, width), bf16),
            dma((len(small),)),
            dma((layers, 3)),
        ]
        + [dma((layers,)), dma((layers, 2))] * 2
        + [dma((layers,)), dma((layers, 2, nc))]
        + [dma((layers,)), dma((layers, 2)), dma((layers,)), dma((layers, 2, 2))]
        + [dma((layers,)), dma((layers, 2, nc))]
        + [dma((1,)), dma((2,)), dma((1,)), dma((2, nc)), dma((1,))]
        + [pltpu.SemaphoreType.REGULAR((3,))],
        compiler_params=pltpu.CompilerParams(
            collective_id=0, has_side_effects=True, vmem_limit_bytes=61 * 2**20
        ),
        cost_estimate=pl.CostEstimate(flops=4 * 10**8, bytes_accessed=10**7, transcendentals=0),
    )(*operands)


def solution(mesh):
    in_specs = (
        P("grp", "cb"),
        P(None, "cb"),
        P(None, "cb", "ra"),
        P(None, "cb", "ra"),
        P(None, "ra"),
        P(None, "ra"),
        P(None, None, "ra"),
        P(None, None, "ra"),
        P(None, "ra", "cb"),
        P(None, "cb"),
    )
    out_specs = P("grp", "cb")
    return jax.shard_map(on_device, mesh=mesh, in_specs=in_specs, out_specs=out_specs, check_vma=False)
```

```python
import functools

import jax
import jax.numpy as jnp
from jax import lax
from jax.experimental import pallas as pl
from jax.experimental.pallas import tpu as pltpu
from jax.sharding import PartitionSpec as P

epsilon = 1e-06
residual_weight = 0.5
MESH = pl.DeviceIdType.MESH
f32 = jnp.float32
bf16 = jnp.bfloat16


def in_three(column):
    hi = column.astype(bf16).astype(f32)
    mid = (column - hi).astype(bf16).astype(f32)
    lo = (column - hi - mid).astype(bf16).astype(f32)
    return hi, mid, lo


def with_lanes(tile, at, columns):
    lane = lax.broadcasted_iota(jnp.int32, tile.shape, 1)
    for k, column in enumerate(columns):
        tile = jnp.where(lane == at + k, column, tile)
    return tile


def as_row(column):
    n = column.shape[0]
    at = lax.broadcasted_iota(jnp.int32, (n, 128), 0) == lax.broadcasted_iota(jnp.int32, (n, 128), 1)
    return jnp.sum(jnp.where(at, column, 0.0), axis=0, keepdims=True)


def as_column(row, n):
    at = lax.broadcasted_iota(jnp.int32, (n, 128), 0) == lax.broadcasted_iota(jnp.int32, (n, 128), 1)
    return jnp.sum(jnp.where(at, row, 0.0), axis=1, keepdims=True)


def kernel(
    dims,
    tok_hbm,
    gains_hbm,
    gate_w,
    value_w,
    gate_scale_hbm,
    value_scale_hbm,
    conv_gate_hbm,
    conv_value_hbm,
    down_w,
    down_scale_hbm,
    out,
    tok,
    gains,
    gate_scale,
    value_scale,
    conv_gate,
    conv_value,
    down_scale,
    raw_in,
    raw_down,
    w_first,
    w_later,
    w_down,
    part,
    part_halo,
    got,
    got_halo,
    pre,
    hid,
    down_part,
    win,
    sums,
    cur,
    squares_row,
    inverse_row,
    result,
    small_sem,
    w_sem,
    ps,
    pr,
    qs,
    qr,
    gs,
    gr,
    zs,
    zr,
    ms,
    mr,
    bs,
    br,
    ns,
    nr,
    vs,
    vr,
    out_sem,
    greeting,
):
    layers, nz, nc, width, ff, ffp, blk, taps = dims
    owners = nz // nc
    half = nc // 2
    rows = blk
    halo = taps - 1
    model_width = width * nc
    z = lax.axis_index("ra")
    c = lax.axis_index("cb")
    mine = lax.rem(z, nc)
    rank = z // nc

    def along_z(d):
        return {"ra": lax.rem(z + d + 2 * nz, nz), "cb": c}

    def along_c(k):
        return {"ra": z, "cb": lax.rem(c + k, nc)}

    def send(src, dst, ssem, rsem, to):
        return pltpu.make_async_remote_copy(
            src_ref=src, dst_ref=dst, send_sem=ssem, recv_sem=rsem, device_id=to, device_id_type=MESH
        )

    barrier = pltpu.get_barrier_semaphore()
    peers = [along_c(k) for k in range(1, nc)] + [along_z(1), along_z(-1)]
    for to in peers:
        pl.semaphore_signal(barrier, inc=1, device_id=to, device_id_type=MESH)

    def greet(stage):
        for d in (-(2**stage), 2**stage):
            pl.semaphore_signal(greeting.at[stage], inc=1, device_id=along_z(d), device_id_type=MESH)

    def greeted(stage):
        pl.semaphore_wait(greeting.at[stage], 2)

    def weight_loads(layer):
        for k, (src, dst) in enumerate(
            (
                (gate_w, raw_in.at[layer, 0, pl.ds(0, ff)]),
                (value_w, raw_in.at[layer, 1, pl.ds(0, ff)]),
                (down_w, raw_down.at[layer]),
            )
        ):
            yield pltpu.make_async_copy(src.at[layer], dst, w_sem.at[layer, k])

    small = [
        pltpu.make_async_copy(src, dst, small_sem.at[k])
        for k, (src, dst) in enumerate(
            (
                (tok_hbm, tok),
                (gains_hbm, gains),
                (gate_scale_hbm, gate_scale),
                (value_scale_hbm, value_scale),
                (conv_gate_hbm, conv_gate),
                (conv_value_hbm, conv_value),
                (down_scale_hbm, down_scale),
            )
        )
    ]
    weights = [list(weight_loads(layer)) for layer in range(layers)]
    for load in small[:2] + weights[0] + small[2:] + sum(weights[1:], []):
        load.start()

    edge = ff // 128 * 128
    for layer in range(layers):
        for s in range(2):
            raw_in[layer, s, ff:, :] = jnp.zeros((ffp - ff, width), f32)
        w_down[layer, ff:, :] = jnp.zeros((ffp - ff, width), bf16)
        part_halo[layer, 0, 0] = jnp.zeros((halo, 2 * ffp), bf16)
        for p in range(2):
            hid[layer, p, c, :, edge:] = jnp.zeros((blk, ffp - edge), bf16)

    def take_in(layer):
        for s in range(2):
            weights[layer][s].wait()
            if layer == 0:
                w_first[s * ffp : (s + 1) * ffp, :] = raw_in[0, s].astype(bf16)
            else:
                w_later[layer - 1, :, s * ffp : (s + 1) * ffp] = raw_in[layer, s].T.astype(bf16)

    def take_down(layer):
        weights[layer][2].wait()
        w_down[layer, 0:ff, :] = raw_down[layer].astype(bf16)

    def partials(x, layer):
        scaled = (x * gains[layer : layer + 1, :]).astype(bf16)
        if layer == 0:
            p = lax.dot_general(scaled, w_first[...], (((1,), (1,)), ((), ())), preferred_element_type=f32)
        else:
            p = jnp.dot(scaled, w_later[layer - 1], preferred_element_type=f32)
        squares = in_three(jnp.sum(x * x, axis=1, keepdims=True))
        last = with_lanes(p[:, edge:ffp], ff - edge, squares)
        return jnp.concatenate([p[:, :edge], last, p[:, ffp:]], axis=1)

    most = pl.ds(0, nc - 1)

    def part_copy(layer, p, b):
        return send(part.at[layer, p, b], got.at[layer, p, c], ps.at[layer], pr.at[layer, p], {"ra": z, "cb": b})

    def part_got(layer, p):
        ref = got.at[layer, p, most]
        return send(ref, ref, ps.at[layer], pr.at[layer, p], along_c(1))

    def part_sent(layer):
        ref = part.at[layer, pl.ds(0, 2), most]
        return send(ref, ref, ps.at[layer], pr.at[layer, 0], along_c(1))

    def halo_copy(layer, p, b):
        return send(
            part_halo.at[layer, p, b], got_halo.at[layer, p, c], qs.at[layer], qr.at[layer, p], {"ra": z, "cb": b}
        )

    def halo_got(layer, p):
        ref = got_halo.at[layer, p, most]
        return send(ref, ref, qs.at[layer], qr.at[layer, p], along_c(1))

    def halo_sent(layer):
        ref = part_halo.at[layer, pl.ds(0, 2), most]
        return send(ref, ref, qs.at[layer], qr.at[layer, 0], along_c(1))

    def hid_copy(layer, p, b, to):
        return send(hid.at[layer, p, b], hid.at[layer, p, b], gs.at[layer], gr.at[layer, p, b], {"ra": z, "cb": to})

    def hid_sent(layer):
        ref = hid.at[layer, pl.ds(0, 2), most]
        return send(ref, ref, gs.at[layer], gr.at[layer, 0, 0], along_c(1))

    here, split = half - 1, nc - 1
    left, right = pl.ds(0, width // 2), pl.ds(width // 2, width // 2)

    def slot_of(b):
        return lax.rem(b - z + here + nz, nc)

    others = [split] + sorted((s for s in range(nc - 1) if s != here), key=lambda s: -abs(s - here))

    def win_copy(layer, p, b, slot):
        return send(
            down_part.at[layer, p, b], win.at[layer, p, slot], zs.at[layer], zr.at[layer, p], along_z(slot - here)
        )

    def win_halves(layer, p, b):
        for columns, d in ((left, half), (right, -half)):
            yield send(
                down_part.at[layer, p, b, :, columns],
                win.at[layer, p, split, :, columns],
                zs.at[layer],
                zr.at[layer, p],
                along_z(d),
            )

    def win_got(layer, p):
        return send(win.at[layer, p, most], win.at[layer, p, most], zs.at[layer], zr.at[layer, p], along_z(1))

    def win_sent(layer):
        ref = down_part.at[layer, pl.ds(0, 2), most]
        return send(ref, ref, zs.at[layer], zr.at[layer, 0], along_z(1))

    upward = nc * (1 - 2 * lax.rem(rank, 2))

    def sum_copies(layer, p, turn):
        for h, sign in enumerate((1, -1) if turn == 0 else (-1, 1)):
            columns = pl.ds(h * (width // 2), width // 2)
            yield send(
                sums.at[layer, p, 2 * turn, :, columns],
                sums.at[layer, p, 2 * turn + 1, :, columns],
                ms.at[layer],
                mr.at[layer, p, turn],
                along_z(sign * upward),
            )

    def sum_got(layer, p, turn):
        ref = sums.at[layer, p, 2 * turn + 1]
        return send(ref, ref, ms.at[layer], mr.at[layer, p, turn], along_z(nc))

    def sum_sent(layer):
        ref = sums.at[layer, pl.ds(0, 2), pl.ds(0, 2)]
        return send(ref, ref, ms.at[layer], mr.at[layer, 0, 0], along_z(nc))

    def cur_copies(layer, p, b):
        for slot in others:
            if slot == split:
                for columns, d in ((left, -half), (right, half)):
                    ref = cur.at[layer, p, b, :, columns]
                    yield send(ref, ref, bs.at[layer], br.at[layer, p, b], along_z(d))
            else:
                ref = cur.at[layer, p, b]
                yield send(ref, ref, bs.at[layer], br.at[layer, p, b], along_z(here - slot))

    def cur_got(layer, p, b):
        ref = cur.at[layer, p, b]
        return send(ref, ref, bs.at[layer], br.at[layer, p, b], along_z(1))

    def cur_sent(layer):
        ref = cur.at[layer, pl.ds(0, 2), most]
        return send(ref, ref, bs.at[layer], br.at[layer, 0, 0], along_z(1))

    def squares_copy(p, to):
        ref = squares_row.at[p, c]
        return send(ref, ref, ns.at[0], nr.at[p], {"ra": z, "cb": to})

    def squares_got(p):
        ref = squares_row.at[p, most]
        return send(ref, ref, ns.at[0], nr.at[p], along_c(1))

    def squares_sent():
        ref = squares_row.at[pl.ds(0, 2), most]
        return send(ref, ref, ns.at[0], nr.at[0], along_c(1))

    def inverse_copy(p, b, slot):
        ref = inverse_row.at[p, b]
        return send(ref, ref, vs.at[0], vr.at[p, b], along_z(here - slot))

    def inverse_got(p, b):
        ref = inverse_row.at[p, b]
        return send(ref, ref, vs.at[0], vr.at[p, b], along_z(1))

    def inverse_sent():
        ref = inverse_row.at[pl.ds(0, 2), most]
        return send(ref, ref, vs.at[0], vr.at[0, 0], along_z(1))

    def near_first(i):
        return (2 * lax.rem(i, 2) - 1) * ((i + 1) // 2)

    far_c = sorted(range(1, nc), key=lambda k: -min(k, nc - k))

    def finish(layer, p, total):
        if layer == 0:
            own = tok[pl.ds(pl.multiple_of((p * nc + mine) * blk, blk), blk), :].astype(f32)
        else:
            own = cur[layer - 1, p, mine].astype(f32)
        new = (residual_weight * own + down_scale[layer : layer + 1, :] * total).astype(bf16)
        if layer == layers - 1:
            wide = new.astype(f32)
            squares_row[p, c] = as_row(jnp.sum(wide * wide, axis=1, keepdims=True))
            for k in far_c:
                squares_copy(p, lax.rem(c + k, nc)).start()
        cur[layer, p, mine] = new
        for copy in cur_copies(layer, p, mine):
            copy.start()

    for layer in range(layers):
        if layer == 0:
            small[0].wait()
            small[1].wait()
            take_in(0)
            before = None
            for p in range(2):
                y = partials(tok[p * nc * blk : (p + 1) * nc * blk, :].astype(f32), 0).reshape(nc, blk, 2 * ffp)
                part[0, p] = y.astype(bf16)
                ends = y[:, blk - halo :, :].astype(bf16)
                if p > 0:
                    part_halo[0, p, 0] = before
                for b in range(1, nc):
                    part_halo[0, p, b] = ends[b - 1]
                before = ends[nc - 1]
                if p == 0:
                    pl.semaphore_wait(barrier, len(peers))
                    greet(0)
                for k in far_c:
                    to = lax.rem(c + k, nc)
                    part_copy(0, p, to).start()
                    halo_copy(0, p, to).start()
        else:
            for p in range(2):
                if p == 0:

                    @pl.when(c != 0)
                    def _(layer=layer):
                        halo_copy(layer, 0, 0).start()

                def two_blocks(i, carry, layer=layer, p=p):
                    b0 = lax.rem(z + near_first(2 * i) + nz, nc)
                    b1 = lax.rem(z + near_first(2 * i + 1) + nz, nc)

                    @pl.when(i > 0)
                    def _():
                        cur_got(layer - 1, p, b0).wait_recv()

                    cur_got(layer - 1, p, b1).wait_recv()
                    x = jnp.concatenate([cur[layer - 1, p, b0], cur[layer - 1, p, b1]], axis=0)
                    y = partials(x.astype(f32), layer)
                    for b, first in ((b0, 0), (b1, blk)):
                        part[layer, p, b] = y[first : first + blk, :].astype(bf16)

                        @pl.when(b != c)
                        def _(b=b):
                            part_copy(layer, p, b).start()

                        ends = y[first + blk - halo : first + blk, :].astype(bf16)
                        after = lax.rem(b + 1, nc)

                        @pl.when(after != 0)
                        def _(after=after, ends=ends):
                            part_halo[layer, p, after] = ends

                            @pl.when(after != c)
                            def _():
                                halo_copy(layer, p, after).start()

                        if p == 0:

                            @pl.when(after == 0)
                            def _(ends=ends):
                                part_halo[layer, 1, 0] = ends

                                @pl.when(c != 0)
                                def _():
                                    halo_copy(layer, 1, 0).start()

                    return carry

                lax.fori_loop(0, nc // 2, two_blocks, 0)

        if layer == 0:
            take_down(0)
            greeted(0)
            greet(1)
            for load in small[2:]:
                load.wait()
            greeted(1)
            greet(2)
        for p in range(2):
            got[layer, p, c] = part[layer, p, c]
            got_halo[layer, p, c] = part_halo[layer, p, c]
            part_got(layer, p).wait_recv()
            halo_got(layer, p).wait_recv()
            for buf, count, at in ((got_halo, halo, 8 - halo), (got, blk, 8)):
                total = buf[layer, p, 0].astype(f32)
                for src in range(1, nc):
                    total = total + buf[layer, p, src].astype(f32)
                squares = jnp.sum(total[:, ff : ff + 3], axis=1, keepdims=True)
                inverse = lax.rsqrt(squares / model_width + epsilon)
                pre[p, at : at + count, 0:ff] = inverse * gate_scale[layer : layer + 1, :] * total[:, 0:ff]
                pre[p, at : at + count, ffp : ffp + ff] = (
                    inverse * value_scale[layer : layer + 1, :] * total[:, ffp : ffp + ff]
                )
            convs = []
            for lane, tap_weights in ((0, conv_gate), (ffp, conv_value)):
                y = None
                for k in range(taps):
                    at = 8 - halo + k
                    term = pre[p, at : at + blk, lane : lane + ff] * tap_weights[k, layer : layer + 1, :]
                    y = term if y is None else y + term
                convs.append(y)
            hid[layer, p, c, :, 0:ff] = (jax.nn.gelu(convs[0], approximate=True) * convs[1]).astype(bf16)
            for k in far_c:
                hid_copy(layer, p, c, lax.rem(c + k, nc)).start()

        for p in range(2):

            def two_downs(i, carry, layer=layer, p=p):
                b0 = lax.rem(c + near_first(2 * i) + nc, nc)
                b1 = lax.rem(c + near_first(2 * i + 1) + nc, nc)

                @pl.when(i > 0)
                def _():
                    hid_copy(layer, p, b0, c).wait_recv()

                hid_copy(layer, p, b1, c).wait_recv()
                h = jnp.concatenate([hid[layer, p, b0], hid[layer, p, b1]], axis=0)
                d = jnp.dot(h, w_down[layer], preferred_element_type=f32).astype(bf16)
                for b, first in ((b0, 0), (b1, blk)):
                    down_part[layer, p, b] = d[first : first + blk, :]
                    slot = slot_of(b)

                    @pl.when(jnp.logical_and(slot != here, slot != split))
                    def _(b=b, slot=slot):
                        win_copy(layer, p, b, slot).start()

                    @pl.when(slot == split)
                    def _(b=b):
                        for copy in win_halves(layer, p, b):
                            copy.start()

                return carry

            lax.fori_loop(0, nc // 2, two_downs, 0)
        if layer + 1 < layers:
            take_in(layer + 1)
            take_down(layer + 1)

        for p in range(2):
            win[layer, p, here] = down_part[layer, p, mine]
            win_got(layer, p).wait_recv()
            total = win[layer, p, 0].astype(f32)
            for slot in range(1, nc):
                total = total + win[layer, p, slot].astype(f32)
            sums[layer, p, 0] = total.astype(bf16)
            if layer == 0 and p == 0:
                greeted(2)
            for copy in sum_copies(layer, p, 0):
                copy.start()
        for turn in range(2):
            for p in range(2):
                sum_got(layer, p, turn).wait_recv()
                both = sums[layer, p, 2 * turn].astype(f32) + sums[layer, p, 2 * turn + 1].astype(f32)
                if turn == 0:
                    sums[layer, p, 2] = both.astype(bf16)
                    for copy in sum_copies(layer, p, 1):
                        copy.start()
                else:
                    finish(layer, p, both)

    for p in range(2):
        squares_got(p).wait_recv()
        total = squares_row[p, 0]
        for k in range(1, nc):
            total = total + squares_row[p, k]
        inverse_row[p, mine] = lax.rsqrt(total / model_width + epsilon)
        for slot in others:
            inverse_copy(p, mine, slot).start()

    last = layers - 1

    def out_copy(p, b):
        there = pl.ds(pl.multiple_of((p * nc + b) * blk, blk), blk)
        return pltpu.make_async_copy(result.at[p, b], out.at[there], out_sem.at[0])

    for p in range(2):

        def put_block(i, carry, p=p):
            b = lax.rem(z + near_first(i) + nz, nc)

            @pl.when(i > 0)
            def _():
                cur_got(last, p, b).wait_recv()
                inverse_got(p, b).wait_recv()

            scale = as_column(inverse_row[p, b], blk)
            wide = cur[last, p, b].astype(f32) * scale * gains[layers : layers + 1, :]
            result[p, b] = wide.astype(bf16)
            out_copy(p, b).start()
            return carry

        lax.fori_loop(0, nc, put_block, 0)

    for layer in range(layers):
        for sent in (part_sent, halo_sent, hid_sent, win_sent, sum_sent, cur_sent):
            sent(layer).wait_send()
    squares_sent().wait_send()
    inverse_sent().wait_send()
    pltpu.make_async_copy(out, out, out_sem.at[0]).wait()


def on_device(
    tokens,
    norm_gains,
    gate_weight,
    value_weight,
    gate_scale,
    value_scale,
    conv_gate,
    conv_value,
    down_weight,
    down_scale,
):
    nz, nc = lax.axis_size("ra"), lax.axis_size("cb")
    rows, width = tokens.shape
    layers, _, ff = gate_weight.shape
    taps = conv_gate.shape[1]
    ffp = (ff + 3 + 127) // 128 * 128
    blk = rows // (2 * nc)
    owners = nz // nc
    dims = (layers, nz, nc, width, ff, ffp, blk, taps)
    dma = pltpu.SemaphoreType.DMA
    operands = (
        tokens,
        norm_gains,
        gate_weight.swapaxes(1, 2),
        value_weight.swapaxes(1, 2),
        gate_scale,
        value_scale,
        conv_gate.swapaxes(0, 1),
        conv_value.swapaxes(0, 1),
        down_weight,
        down_scale,
    )
    small = [operands[k] for k in (0, 1, 4, 5, 6, 7, 9)]
    return pl.pallas_call(
        functools.partial(kernel, dims),
        out_shape=jax.ShapeDtypeStruct((rows, width), bf16),
        in_specs=[pl.BlockSpec(memory_space=pltpu.HBM)] * len(operands),
        out_specs=pl.BlockSpec(memory_space=pltpu.HBM),
        scratch_shapes=[pltpu.VMEM(a.shape, a.dtype) for a in small]
        + [
            pltpu.VMEM((layers, 2, ffp, width), f32),
            pltpu.VMEM((layers, ff, width), f32),
            pltpu.VMEM((2 * ffp, width), bf16),
            pltpu.VMEM((layers - 1, width, 2 * ffp), bf16),
            pltpu.VMEM((layers, ffp, width), bf16),
            pltpu.VMEM((layers, 2, nc, blk, 2 * ffp), bf16),
            pltpu.VMEM((layers, 2, nc, taps - 1, 2 * ffp), bf16),
            pltpu.VMEM((layers, 2, nc, blk, 2 * ffp), bf16),
            pltpu.VMEM((layers, 2, nc, taps - 1, 2 * ffp), bf16),
            pltpu.VMEM((2, 8 + blk, 2 * ffp), f32),
            pltpu.VMEM((layers, 2, nc, blk, ffp), bf16),
            pltpu.VMEM((layers, 2, nc, blk, width), bf16),
            pltpu.VMEM((layers, 2, nc, blk, width), bf16),
            pltpu.VMEM((layers, 2, owners, blk, width), bf16),
            pltpu.VMEM((layers, 2, nc, blk, width), bf16),
            pltpu.VMEM((2, nc, 1, 128), f32),
            pltpu.VMEM((2, nc, 1, 128), f32),
            pltpu.VMEM((2, nc, blk, width), bf16),
            dma((len(small),)),
            dma((layers, 3)),
        ]
        + [dma((layers,)), dma((layers, 2))] * 2
        + [dma((layers,)), dma((layers, 2, nc))]
        + [dma((layers,)), dma((layers, 2)), dma((layers,)), dma((layers, 2, 2))]
        + [dma((layers,)), dma((layers, 2, nc))]
        + [dma((1,)), dma((2,)), dma((1,)), dma((2, nc)), dma((1,))]
        + [pltpu.SemaphoreType.REGULAR((3,))],
        compiler_params=pltpu.CompilerParams(
            collective_id=0, has_side_effects=True, vmem_limit_bytes=61 * 2**20
        ),
        cost_estimate=pl.CostEstimate(flops=4 * 10**8, bytes_accessed=10**7, transcendentals=0),
    )(*operands)


def solution(mesh):
    in_specs = (
        P("grp", "cb"),
        P(None, "cb"),
        P(None, "cb", "ra"),
        P(None, "cb", "ra"),
        P(None, "ra"),
        P(None, "ra"),
        P(None, None, "ra"),
        P(None, None, "ra"),
        P(None, "ra", "cb"),
        P(None, "cb"),
    )
    out_specs = P("grp", "cb")
    return jax.shard_map(on_device, mesh=mesh, in_specs=in_specs, out_specs=out_specs, check_vma=False)
```

```python
import functools

import jax
import jax.numpy as jnp
from jax import lax
from jax.experimental import pallas as pl
from jax.experimental.pallas import tpu as pltpu
from jax.sharding import PartitionSpec as P

epsilon = 1e-06
residual_weight = 0.5
MESH = pl.DeviceIdType.MESH
f32 = jnp.float32
bf16 = jnp.bfloat16


def in_three(column):
    hi = column.astype(bf16).astype(f32)
    mid = (column - hi).astype(bf16).astype(f32)
    lo = (column - hi - mid).astype(bf16).astype(f32)
    return hi, mid, lo


def with_lanes(tile, at, columns):
    lane = lax.broadcasted_iota(jnp.int32, tile.shape, 1)
    for k, column in enumerate(columns):
        tile = jnp.where(lane == at + k, column, tile)
    return tile


def as_row(column):
    n = column.shape[0]
    at = lax.broadcasted_iota(jnp.int32, (n, 128), 0) == lax.broadcasted_iota(jnp.int32, (n, 128), 1)
    return jnp.sum(jnp.where(at, column, 0.0), axis=0, keepdims=True)


def as_column(row, n):
    at = lax.broadcasted_iota(jnp.int32, (n, 128), 0) == lax.broadcasted_iota(jnp.int32, (n, 128), 1)
    return jnp.sum(jnp.where(at, row, 0.0), axis=1, keepdims=True)


def kernel(
    dims,
    tok_hbm,
    gains_hbm,
    gate_w,
    value_w,
    gate_scale_hbm,
    value_scale_hbm,
    conv_gate_hbm,
    conv_value_hbm,
    down_w,
    down_scale_hbm,
    out,
    tok,
    gains,
    gate_scale,
    value_scale,
    conv_gate,
    conv_value,
    down_scale,
    raw_in,
    raw_down,
    w_first,
    w_later,
    w_down,
    part,
    part_halo,
    got,
    got_halo,
    pre,
    hid,
    down_part,
    win,
    sums,
    cur,
    squares_row,
    inverse_row,
    result,
    small_sem,
    w_sem,
    ps,
    pr,
    qs,
    qr,
    gs,
    gr,
    zs,
    zr,
    ms,
    mr,
    bs,
    br,
    ns,
    nr,
    vs,
    vr,
    out_sem,
    greeting,
):
    layers, nz, nc, width, ff, ffp, blk, taps = dims
    owners = nz // nc
    half = nc // 2
    rows = blk
    halo = taps - 1
    model_width = width * nc
    z = lax.axis_index("ra")
    c = lax.axis_index("cb")
    mine = lax.rem(z, nc)
    rank = z // nc

    def along_z(d):
        return {"ra": lax.rem(z + d + 2 * nz, nz), "cb": c}

    def along_c(k):
        return {"ra": z, "cb": lax.rem(c + k, nc)}

    def send(src, dst, ssem, rsem, to):
        return pltpu.make_async_remote_copy(
            src_ref=src, dst_ref=dst, send_sem=ssem, recv_sem=rsem, device_id=to, device_id_type=MESH
        )

    barrier = pltpu.get_barrier_semaphore()
    peers = [along_c(k) for k in range(1, nc)] + [along_z(1), along_z(-1)]
    for to in peers:
        pl.semaphore_signal(barrier, inc=1, device_id=to, device_id_type=MESH)

    def greet(stage):
        for d in (-(2**stage), 2**stage):
            pl.semaphore_signal(greeting.at[stage], inc=1, device_id=along_z(d), device_id_type=MESH)

    def greeted(stage):
        pl.semaphore_wait(greeting.at[stage], 2)

    def weight_loads(layer):
        for k, (src, dst) in enumerate(
            (
                (gate_w, raw_in.at[layer, 0, pl.ds(0, ff)]),
                (value_w, raw_in.at[layer, 1, pl.ds(0, ff)]),
                (down_w, raw_down.at[layer]),
            )
        ):
            yield pltpu.make_async_copy(src.at[layer], dst, w_sem.at[layer, k])

    small = [
        pltpu.make_async_copy(src, dst, small_sem.at[k])
        for k, (src, dst) in enumerate(
            (
                (tok_hbm, tok),
                (gains_hbm, gains),
                (gate_scale_hbm, gate_scale),
                (value_scale_hbm, value_scale),
                (conv_gate_hbm, conv_gate),
                (conv_value_hbm, conv_value),
                (down_scale_hbm, down_scale),
            )
        )
    ]
    weights = [list(weight_loads(layer)) for layer in range(layers)]
    for load in small[:2] + weights[0] + small[2:] + sum(weights[1:], []):
        load.start()

    edge = ff // 128 * 128
    for layer in range(layers):
        for s in range(2):
            raw_in[layer, s, ff:, :] = jnp.zeros((ffp - ff, width), f32)
        w_down[layer, ff:, :] = jnp.zeros((ffp - ff, width), bf16)
        part_halo[layer, 0, 0] = jnp.zeros((halo, 2 * ffp), bf16)
        for p in range(2):
            hid[layer, p, c, :, edge:] = jnp.zeros((blk, ffp - edge), bf16)

    def take_in(layer):
        for s in range(2):
            weights[layer][s].wait()
            if layer == 0:
                w_first[s * ffp : (s + 1) * ffp, :] = raw_in[0, s].astype(bf16)
            else:
                w_later[layer - 1, :, s * ffp : (s + 1) * ffp] = raw_in[layer, s].T.astype(bf16)

    def take_down(layer):
        weights[layer][2].wait()
        w_down[layer, 0:ff, :] = raw_down[layer].astype(bf16)

    def partials(x, layer):
        scaled = (x * gains[layer : layer + 1, :]).astype(bf16)
        if layer == 0:
            p = lax.dot_general(scaled, w_first[...], (((1,), (1,)), ((), ())), preferred_element_type=f32)
        else:
            p = jnp.dot(scaled, w_later[layer - 1], preferred_element_type=f32)
        squares = in_three(jnp.sum(x * x, axis=1, keepdims=True))
        last = with_lanes(p[:, edge:ffp], ff - edge, squares)
        return jnp.concatenate([p[:, :edge], last, p[:, ffp:]], axis=1)

    most = pl.ds(0, nc - 1)

    def part_copy(layer, p, b):
        return send(part.at[layer, p, b], got.at[layer, p, c], ps.at[layer], pr.at[layer, p], {"ra": z, "cb": b})

    def part_got(layer, p):
        ref = got.at[layer, p, most]
        return send(ref, ref, ps.at[layer], pr.at[layer, p], along_c(1))

    def part_sent(layer):
        ref = part.at[layer, pl.ds(0, 2), most]
        return send(ref, ref, ps.at[layer], pr.at[layer, 0], along_c(1))

    def halo_copy(layer, p, b):
        return send(
            part_halo.at[layer, p, b], got_halo.at[layer, p, c], qs.at[layer], qr.at[layer, p], {"ra": z, "cb": b}
        )

    def halo_got(layer, p):
        ref = got_halo.at[layer, p, most]
        return send(ref, ref, qs.at[layer], qr.at[layer, p], along_c(1))

    def halo_sent(layer):
        ref = part_halo.at[layer, pl.ds(0, 2), most]
        return send(ref, ref, qs.at[layer], qr.at[layer, 0], along_c(1))

    def hid_copy(layer, p, b, to):
        return send(hid.at[layer, p, b], hid.at[layer, p, b], gs.at[layer], gr.at[layer, p, b], {"ra": z, "cb": to})

    def hid_sent(layer):
        ref = hid.at[layer, pl.ds(0, 2), most]
        return send(ref, ref, gs.at[layer], gr.at[layer, 0, 0], along_c(1))

    here, split = half - 1, nc - 1
    sides = (pl.ds(0, width // 2), pl.ds(width // 2, width // 2))
    side = (slice(0, width // 2), slice(width // 2, width))

    def slot_of(b):
        return lax.rem(b - z + here + nz, nc)

    others = [split] + sorted((s for s in range(nc - 1) if s != here), key=lambda s: -abs(s - here))

    def win_copy(layer, p, h, b, slot, d):
        return send(
            down_part.at[layer, p, b, :, sides[h]],
            win.at[layer, p, slot, :, sides[h]],
            zs.at[layer],
            zr.at[layer, p, h],
            along_z(d),
        )

    def win_got(layer, p, h):
        ref = win.at[layer, p, most, :, sides[h]]
        return send(ref, ref, zs.at[layer], zr.at[layer, p, h], along_z(1))

    def win_sent(layer):
        ref = down_part.at[layer, pl.ds(0, 2), most]
        return send(ref, ref, zs.at[layer], zr.at[layer, 0, 0], along_z(1))

    upward = nc * (1 - 2 * lax.rem(rank, 2))

    def sum_copy(layer, p, h, turn):
        return send(
            sums.at[layer, p, 2 * turn, :, sides[h]],
            sums.at[layer, p, 2 * turn + 1, :, sides[h]],
            ms.at[layer],
            mr.at[layer, p, h, turn],
            along_z(upward if h == turn else -upward),
        )

    def sum_got(layer, p, h, turn):
        ref = sums.at[layer, p, 2 * turn + 1, :, sides[h]]
        return send(ref, ref, ms.at[layer], mr.at[layer, p, h, turn], along_z(nc))

    def sum_sent(layer):
        ref = sums.at[layer, pl.ds(0, 2), pl.ds(0, 2)]
        return send(ref, ref, ms.at[layer], mr.at[layer, 0, 0, 0], along_z(nc))

    def cur_copies(layer, p, h, b):
        for slot in others:
            ref = cur.at[layer, p, b, :, sides[h]]
            d = here - slot + (nc if slot == split and h == 1 else 0)
            yield send(ref, ref, bs.at[layer], br.at[layer, p, b], along_z(d))

    def cur_got(layer, p, b):
        ref = cur.at[layer, p, b]
        return send(ref, ref, bs.at[layer], br.at[layer, p, b], along_z(1))

    def cur_sent(layer):
        ref = cur.at[layer, pl.ds(0, 2), most]
        return send(ref, ref, bs.at[layer], br.at[layer, 0, 0], along_z(1))

    def squares_copy(p, to):
        ref = squares_row.at[p, c]
        return send(ref, ref, ns.at[0], nr.at[p], {"ra": z, "cb": to})

    def squares_got(p):
        ref = squares_row.at[p, most]
        return send(ref, ref, ns.at[0], nr.at[p], along_c(1))

    def squares_sent():
        ref = squares_row.at[pl.ds(0, 2), most]
        return send(ref, ref, ns.at[0], nr.at[0], along_c(1))

    def inverse_copy(p, b, slot):
        ref = inverse_row.at[p, b]
        return send(ref, ref, vs.at[0], vr.at[p, b], along_z(here - slot))

    def inverse_got(p, b):
        ref = inverse_row.at[p, b]
        return send(ref, ref, vs.at[0], vr.at[p, b], along_z(1))

    def inverse_sent():
        ref = inverse_row.at[pl.ds(0, 2), most]
        return send(ref, ref, vs.at[0], vr.at[0, 0], along_z(1))

    def near_first(i):
        return (2 * lax.rem(i, 2) - 1) * ((i + 1) // 2)

    far_c = sorted(range(1, nc), key=lambda k: -min(k, nc - k))

    lengths = {}

    def finish(layer, p, h, total):
        if layer == 0:
            there = pl.ds(pl.multiple_of((p * nc + mine) * blk, blk), blk)
            own = tok[there, side[h]].astype(f32)
        else:
            own = cur[layer - 1, p, mine, :, side[h]].astype(f32)
        new = (residual_weight * own + down_scale[layer : layer + 1, side[h]] * total).astype(bf16)
        if layer == layers - 1:
            wide = new.astype(f32)
            lengths[p, h] = jnp.sum(wide * wide, axis=1, keepdims=True)
            if h == 1:
                squares_row[p, c] = as_row(lengths[p, 0] + lengths[p, 1])
                for k in far_c:
                    squares_copy(p, lax.rem(c + k, nc)).start()
        cur[layer, p, mine, :, side[h]] = new
        for copy in cur_copies(layer, p, h, mine):
            copy.start()

    for layer in range(layers):
        if layer == 0:
            small[0].wait()
            small[1].wait()
            take_in(0)
            before = None
            for p in range(2):
                y = partials(tok[p * nc * blk : (p + 1) * nc * blk, :].astype(f32), 0).reshape(nc, blk, 2 * ffp)
                part[0, p] = y.astype(bf16)
                ends = y[:, blk - halo :, :].astype(bf16)
                if p > 0:
                    part_halo[0, p, 0] = before
                for b in range(1, nc):
                    part_halo[0, p, b] = ends[b - 1]
                before = ends[nc - 1]
                if p == 0:
                    pl.semaphore_wait(barrier, len(peers))
                    greet(0)
                for k in far_c:
                    to = lax.rem(c + k, nc)
                    part_copy(0, p, to).start()
                    halo_copy(0, p, to).start()
        else:
            for p in range(2):
                if p == 0:

                    @pl.when(c != 0)
                    def _(layer=layer):
                        halo_copy(layer, 0, 0).start()

                def two_blocks(i, carry, layer=layer, p=p):
                    b0 = lax.rem(z + near_first(2 * i) + nz, nc)
                    b1 = lax.rem(z + near_first(2 * i + 1) + nz, nc)

                    @pl.when(i > 0)
                    def _():
                        cur_got(layer - 1, p, b0).wait_recv()

                    cur_got(layer - 1, p, b1).wait_recv()
                    x = jnp.concatenate([cur[layer - 1, p, b0], cur[layer - 1, p, b1]], axis=0)
                    y = partials(x.astype(f32), layer)
                    for b, first in ((b0, 0), (b1, blk)):
                        part[layer, p, b] = y[first : first + blk, :].astype(bf16)

                        @pl.when(b != c)
                        def _(b=b):
                            part_copy(layer, p, b).start()

                        ends = y[first + blk - halo : first + blk, :].astype(bf16)
                        after = lax.rem(b + 1, nc)

                        @pl.when(after != 0)
                        def _(after=after, ends=ends):
                            part_halo[layer, p, after] = ends

                            @pl.when(after != c)
                            def _():
                                halo_copy(layer, p, after).start()

                        if p == 0:

                            @pl.when(after == 0)
                            def _(ends=ends):
                                part_halo[layer, 1, 0] = ends

                                @pl.when(c != 0)
                                def _():
                                    halo_copy(layer, 1, 0).start()

                    return carry

                lax.fori_loop(0, nc // 2, two_blocks, 0)

        if layer == 0:
            take_down(0)
            greeted(0)
            greet(1)
            for load in small[2:]:
                load.wait()
            greeted(1)
            greet(2)
        for p in range(2):
            got[layer, p, c] = part[layer, p, c]
            got_halo[layer, p, c] = part_halo[layer, p, c]
            part_got(layer, p).wait_recv()
            halo_got(layer, p).wait_recv()
            for buf, count, at in ((got_halo, halo, 8 - halo), (got, blk, 8)):
                total = buf[layer, p, 0].astype(f32)
                for src in range(1, nc):
                    total = total + buf[layer, p, src].astype(f32)
                squares = jnp.sum(total[:, ff : ff + 3], axis=1, keepdims=True)
                inverse = lax.rsqrt(squares / model_width + epsilon)
                pre[p, at : at + count, 0:ff] = inverse * gate_scale[layer : layer + 1, :] * total[:, 0:ff]
                pre[p, at : at + count, ffp : ffp + ff] = (
                    inverse * value_scale[layer : layer + 1, :] * total[:, ffp : ffp + ff]
                )
            convs = []
            for lane, tap_weights in ((0, conv_gate), (ffp, conv_value)):
                y = None
                for k in range(taps):
                    at = 8 - halo + k
                    term = pre[p, at : at + blk, lane : lane + ff] * tap_weights[k, layer : layer + 1, :]
                    y = term if y is None else y + term
                convs.append(y)
            hid[layer, p, c, :, 0:ff] = (jax.nn.gelu(convs[0], approximate=True) * convs[1]).astype(bf16)
            for k in far_c:
                hid_copy(layer, p, c, lax.rem(c + k, nc)).start()

        for p in range(2):

            def two_downs(i, carry, layer=layer, p=p):
                b0 = lax.rem(c + near_first(2 * i) + nc, nc)
                b1 = lax.rem(c + near_first(2 * i + 1) + nc, nc)

                @pl.when(i > 0)
                def _():
                    hid_copy(layer, p, b0, c).wait_recv()

                hid_copy(layer, p, b1, c).wait_recv()
                h = jnp.concatenate([hid[layer, p, b0], hid[layer, p, b1]], axis=0)
                d = jnp.dot(h, w_down[layer], preferred_element_type=f32).astype(bf16)
                for b, first in ((b0, 0), (b1, blk)):
                    down_part[layer, p, b] = d[first : first + blk, :]
                    slot = slot_of(b)

                    @pl.when(slot != here)
                    def _(b=b, slot=slot):
                        win_copy(layer, p, 0, b, slot, slot - here).start()

                return carry

            lax.fori_loop(0, nc // 2, two_downs, 0)
            for slot in others:
                b = lax.rem(z + slot - here + nz, nc)
                win_copy(layer, p, 1, b, slot, slot - here - (nc if slot == split else 0)).start()
        if layer + 1 < layers:
            take_in(layer + 1)
            take_down(layer + 1)

        pieces = [(p, h) for p in range(2) for h in range(2)]
        for p, h in pieces:
            if h == 0:
                win[layer, p, here] = down_part[layer, p, mine]
            win_got(layer, p, h).wait_recv()
            total = win[layer, p, 0, :, side[h]].astype(f32)
            for slot in range(1, nc):
                total = total + win[layer, p, slot, :, side[h]].astype(f32)
            sums[layer, p, 0, :, side[h]] = total.astype(bf16)
            if layer == 0 and (p, h) == (0, 0):
                greeted(2)
            sum_copy(layer, p, h, 0).start()
        for turn in range(2):
            for p, h in pieces:
                sum_got(layer, p, h, turn).wait_recv()
                both = sums[layer, p, 2 * turn, :, side[h]].astype(f32)
                both = both + sums[layer, p, 2 * turn + 1, :, side[h]].astype(f32)
                if turn == 0:
                    sums[layer, p, 2, :, side[h]] = both.astype(bf16)
                    sum_copy(layer, p, h, 1).start()
                else:
                    finish(layer, p, h, both)

    for p in range(2):
        squares_got(p).wait_recv()
        total = squares_row[p, 0]
        for k in range(1, nc):
            total = total + squares_row[p, k]
        inverse_row[p, mine] = lax.rsqrt(total / model_width + epsilon)
        for slot in others:
            inverse_copy(p, mine, slot).start()

    last = layers - 1

    def out_copy(p, b):
        there = pl.ds(pl.multiple_of((p * nc + b) * blk, blk), blk)
        return pltpu.make_async_copy(result.at[p, b], out.at[there], out_sem.at[0])

    for p in range(2):

        def put_block(i, carry, p=p):
            b = lax.rem(z + near_first(i) + nz, nc)

            @pl.when(i > 0)
            def _():
                cur_got(last, p, b).wait_recv()
                inverse_got(p, b).wait_recv()

            scale = as_column(inverse_row[p, b], blk)
            wide = cur[last, p, b].astype(f32) * scale * gains[layers : layers + 1, :]
            result[p, b] = wide.astype(bf16)
            out_copy(p, b).start()
            return carry

        lax.fori_loop(0, nc, put_block, 0)

    for layer in range(layers):
        for sent in (part_sent, halo_sent, hid_sent, win_sent, sum_sent, cur_sent):
            sent(layer).wait_send()
    squares_sent().wait_send()
    inverse_sent().wait_send()
    pltpu.make_async_copy(out, out, out_sem.at[0]).wait()


def on_device(
    tokens,
    norm_gains,
    gate_weight,
    value_weight,
    gate_scale,
    value_scale,
    conv_gate,
    conv_value,
    down_weight,
    down_scale,
):
    nz, nc = lax.axis_size("ra"), lax.axis_size("cb")
    rows, width = tokens.shape
    layers, _, ff = gate_weight.shape
    taps = conv_gate.shape[1]
    ffp = (ff + 3 + 127) // 128 * 128
    blk = rows // (2 * nc)
    owners = nz // nc
    dims = (layers, nz, nc, width, ff, ffp, blk, taps)
    dma = pltpu.SemaphoreType.DMA
    operands = (
        tokens,
        norm_gains,
        gate_weight.swapaxes(1, 2),
        value_weight.swapaxes(1, 2),
        gate_scale,
        value_scale,
        conv_gate.swapaxes(0, 1),
        conv_value.swapaxes(0, 1),
        down_weight,
        down_scale,
    )
    small = [operands[k] for k in (0, 1, 4, 5, 6, 7, 9)]
    return pl.pallas_call(
        functools.partial(kernel, dims),
        out_shape=jax.ShapeDtypeStruct((rows, width), bf16),
        in_specs=[pl.BlockSpec(memory_space=pltpu.HBM)] * len(operands),
        out_specs=pl.BlockSpec(memory_space=pltpu.HBM),
        scratch_shapes=[pltpu.VMEM(a.shape, a.dtype) for a in small]
        + [
            pltpu.VMEM((layers, 2, ffp, width), f32),
            pltpu.VMEM((layers, ff, width), f32),
            pltpu.VMEM((2 * ffp, width), bf16),
            pltpu.VMEM((layers - 1, width, 2 * ffp), bf16),
            pltpu.VMEM((layers, ffp, width), bf16),
            pltpu.VMEM((layers, 2, nc, blk, 2 * ffp), bf16),
            pltpu.VMEM((layers, 2, nc, taps - 1, 2 * ffp), bf16),
            pltpu.VMEM((layers, 2, nc, blk, 2 * ffp), bf16),
            pltpu.VMEM((layers, 2, nc, taps - 1, 2 * ffp), bf16),
            pltpu.VMEM((2, 8 + blk, 2 * ffp), f32),
            pltpu.VMEM((layers, 2, nc, blk, ffp), bf16),
            pltpu.VMEM((layers, 2, nc, blk, width), bf16),
            pltpu.VMEM((layers, 2, nc, blk, width), bf16),
            pltpu.VMEM((layers, 2, owners, blk, width), bf16),
            pltpu.VMEM((layers, 2, nc, blk, width), bf16),
            pltpu.VMEM((2, nc, 1, 128), f32),
            pltpu.VMEM((2, nc, 1, 128), f32),
            pltpu.VMEM((2, nc, blk, width), bf16),
            dma((len(small),)),
            dma((layers, 3)),
        ]
        + [dma((layers,)), dma((layers, 2))] * 2
        + [dma((layers,)), dma((layers, 2, nc))]
        + [dma((layers,)), dma((layers, 2, 2)), dma((layers,)), dma((layers, 2, 2, 2))]
        + [dma((layers,)), dma((layers, 2, nc))]
        + [dma((1,)), dma((2,)), dma((1,)), dma((2, nc)), dma((1,))]
        + [pltpu.SemaphoreType.REGULAR((3,))],
        compiler_params=pltpu.CompilerParams(
            collective_id=0, has_side_effects=True, vmem_limit_bytes=61 * 2**20
        ),
        cost_estimate=pl.CostEstimate(flops=4 * 10**8, bytes_accessed=10**7, transcendentals=0),
    )(*operands)


def solution(mesh):
    in_specs = (
        P("grp", "cb"),
        P(None, "cb"),
        P(None, "cb", "ra"),
        P(None, "cb", "ra"),
        P(None, "ra"),
        P(None, "ra"),
        P(None, None, "ra"),
        P(None, None, "ra"),
        P(None, "ra", "cb"),
        P(None, "cb"),
    )
    out_specs = P("grp", "cb")
    return jax.shard_map(on_device, mesh=mesh, in_specs=in_specs, out_specs=out_specs, check_vma=False)
```

```python
import functools

import jax
import jax.numpy as jnp
from jax import lax
from jax.experimental import pallas as pl
from jax.experimental.pallas import tpu as pltpu
from jax.sharding import PartitionSpec as P

epsilon = 1e-06
residual_weight = 0.5
MESH = pl.DeviceIdType.MESH
f32 = jnp.float32
bf16 = jnp.bfloat16


def in_three(column):
    hi = column.astype(bf16).astype(f32)
    mid = (column - hi).astype(bf16).astype(f32)
    lo = (column - hi - mid).astype(bf16).astype(f32)
    return hi, mid, lo


def with_lanes(tile, at, columns):
    lane = lax.broadcasted_iota(jnp.int32, tile.shape, 1)
    for k, column in enumerate(columns):
        tile = jnp.where(lane == at + k, column, tile)
    return tile


def as_row(column):
    n = column.shape[0]
    at = lax.broadcasted_iota(jnp.int32, (n, 128), 0) == lax.broadcasted_iota(jnp.int32, (n, 128), 1)
    return jnp.sum(jnp.where(at, column, 0.0), axis=0, keepdims=True)


def as_column(row, n):
    at = lax.broadcasted_iota(jnp.int32, (n, 128), 0) == lax.broadcasted_iota(jnp.int32, (n, 128), 1)
    return jnp.sum(jnp.where(at, row, 0.0), axis=1, keepdims=True)


def kernel(
    dims,
    tok_hbm,
    gains_hbm,
    gate_w,
    value_w,
    gate_scale_hbm,
    value_scale_hbm,
    conv_gate_hbm,
    conv_value_hbm,
    down_w,
    down_scale_hbm,
    out,
    tok,
    gains,
    gate_scale,
    value_scale,
    conv_gate,
    conv_value,
    down_scale,
    raw_in,
    raw_down,
    w_first,
    w_later,
    w_down,
    part,
    part_halo,
    got,
    got_halo,
    pre,
    hid,
    down_part,
    win,
    sums,
    cur,
    squares_row,
    inverse_row,
    result,
    small_sem,
    w_sem,
    ps,
    pr,
    qs,
    qr,
    gs,
    gr,
    zs,
    zr,
    ms,
    mr,
    bs,
    br,
    ns,
    nr,
    vs,
    vr,
    out_sem,
    greeting,
):
    layers, nz, nc, width, ff, ffp, blk, taps = dims
    owners = nz // nc
    half = nc // 2
    rows = blk
    halo = taps - 1
    model_width = width * nc
    z = lax.axis_index("ra")
    c = lax.axis_index("cb")
    mine = lax.rem(z, nc)
    rank = z // nc

    def along_z(d):
        return {"ra": lax.rem(z + d + 2 * nz, nz), "cb": c}

    def along_c(k):
        return {"ra": z, "cb": lax.rem(c + k, nc)}

    def send(src, dst, ssem, rsem, to):
        return pltpu.make_async_remote_copy(
            src_ref=src, dst_ref=dst, send_sem=ssem, recv_sem=rsem, device_id=to, device_id_type=MESH
        )

    barrier = pltpu.get_barrier_semaphore()
    peers = [along_c(k) for k in range(1, nc)] + [along_z(1), along_z(-1)]
    for to in peers:
        pl.semaphore_signal(barrier, inc=1, device_id=to, device_id_type=MESH)

    def greet(stage):
        for d in (-(2**stage), 2**stage):
            pl.semaphore_signal(greeting.at[stage], inc=1, device_id=along_z(d), device_id_type=MESH)

    def greeted(stage):
        pl.semaphore_wait(greeting.at[stage], 2)

    def weight_loads(layer):
        for k, (src, dst) in enumerate(
            (
                (gate_w, raw_in.at[layer, 0, pl.ds(0, ff)]),
                (value_w, raw_in.at[layer, 1, pl.ds(0, ff)]),
                (down_w, raw_down.at[layer]),
            )
        ):
            yield pltpu.make_async_copy(src.at[layer], dst, w_sem.at[layer, k])

    small = [
        pltpu.make_async_copy(src, dst, small_sem.at[k])
        for k, (src, dst) in enumerate(
            (
                (tok_hbm, tok),
                (gains_hbm, gains),
                (gate_scale_hbm, gate_scale),
                (value_scale_hbm, value_scale),
                (conv_gate_hbm, conv_gate),
                (conv_value_hbm, conv_value),
                (down_scale_hbm, down_scale),
            )
        )
    ]
    weights = [list(weight_loads(layer)) for layer in range(layers)]
    for load in small[:2] + weights[0] + small[2:] + sum(weights[1:], []):
        load.start()

    edge = ff // 128 * 128
    for layer in range(layers):
        for s in range(2):
            raw_in[layer, s, ff:, :] = jnp.zeros((ffp - ff, width), f32)
        w_down[layer, ff:, :] = jnp.zeros((ffp - ff, width), bf16)
        part_halo[layer, 0, 0] = jnp.zeros((halo, 2 * ffp), bf16)
        for p in range(2):
            hid[layer, p, c, :, edge:] = jnp.zeros((blk, ffp - edge), bf16)

    def take_in(layer):
        for s in range(2):
            weights[layer][s].wait()
            if layer == 0:
                w_first[s * ffp : (s + 1) * ffp, :] = raw_in[0, s].astype(bf16)
            else:
                w_later[layer - 1, :, s * ffp : (s + 1) * ffp] = raw_in[layer, s].T.astype(bf16)

    def take_down(layer):
        weights[layer][2].wait()
        w_down[layer, 0:ff, :] = raw_down[layer].astype(bf16)

    def partials(x, layer):
        scaled = (x * gains[layer : layer + 1, :]).astype(bf16)
        if layer == 0:
            p = lax.dot_general(scaled, w_first[...], (((1,), (1,)), ((), ())), preferred_element_type=f32)
        else:
            p = jnp.dot(scaled, w_later[layer - 1], preferred_element_type=f32)
        squares = in_three(jnp.sum(x * x, axis=1, keepdims=True))
        last = with_lanes(p[:, edge:ffp], ff - edge, squares)
        return jnp.concatenate([p[:, :edge], last, p[:, ffp:]], axis=1)

    most = pl.ds(0, nc - 1)

    def part_copy(layer, p, b):
        return send(part.at[layer, p, b], got.at[layer, p, c], ps.at[layer], pr.at[layer, p], {"ra": z, "cb": b})

    def part_got(layer, p):
        ref = got.at[layer, p, most]
        return send(ref, ref, ps.at[layer], pr.at[layer, p], along_c(1))

    def part_sent(layer):
        ref = part.at[layer, pl.ds(0, 2), most]
        return send(ref, ref, ps.at[layer], pr.at[layer, 0], along_c(1))

    def halo_copy(layer, p, b):
        return send(
            part_halo.at[layer, p, b], got_halo.at[layer, p, c], qs.at[layer], qr.at[layer, p], {"ra": z, "cb": b}
        )

    def halo_got(layer, p):
        ref = got_halo.at[layer, p, most]
        return send(ref, ref, qs.at[layer], qr.at[layer, p], along_c(1))

    def halo_sent(layer):
        ref = part_halo.at[layer, pl.ds(0, 2), most]
        return send(ref, ref, qs.at[layer], qr.at[layer, 0], along_c(1))

    def hid_copy(layer, p, b, to):
        return send(hid.at[layer, p, b], hid.at[layer, p, b], gs.at[layer], gr.at[layer, p, b], {"ra": z, "cb": to})

    def hid_sent(layer):
        ref = hid.at[layer, pl.ds(0, 2), most]
        return send(ref, ref, gs.at[layer], gr.at[layer, 0, 0], along_c(1))

    here, split = half - 1, nc - 1
    left, right = pl.ds(0, width // 2), pl.ds(width // 2, width // 2)

    def slot_of(b):
        return lax.rem(b - z + here + nz, nc)

    others = [split] + sorted((s for s in range(nc - 1) if s != here), key=lambda s: -abs(s - here))

    def win_copy(layer, p, b, slot):
        return send(
            down_part.at[layer, p, b], win.at[layer, p, slot], zs.at[layer], zr.at[layer, p], along_z(slot - here)
        )

    def win_halves(layer, p, b):
        for columns, d in ((left, half), (right, -half)):
            yield send(
                down_part.at[layer, p, b, :, columns],
                win.at[layer, p, split, :, columns],
                zs.at[layer],
                zr.at[layer, p],
                along_z(d),
            )

    def win_got(layer, p):
        return send(win.at[layer, p, most], win.at[layer, p, most], zs.at[layer], zr.at[layer, p], along_z(1))

    def win_sent(layer):
        ref = down_part.at[layer, pl.ds(0, 2), most]
        return send(ref, ref, zs.at[layer], zr.at[layer, 0], along_z(1))

    upward = nc * (1 - 2 * lax.rem(rank, 2))

    def sum_copies(layer, p, turn):
        for h, sign in enumerate((1, -1) if turn == 0 else (-1, 1)):
            columns = pl.ds(h * (width // 2), width // 2)
            yield send(
                sums.at[layer, p, 2 * turn, :, columns],
                sums.at[layer, p, 2 * turn + 1, :, columns],
                ms.at[layer],
                mr.at[layer, p, turn],
                along_z(sign * upward),
            )

    def sum_got(layer, p, turn):
        ref = sums.at[layer, p, 2 * turn + 1]
        return send(ref, ref, ms.at[layer], mr.at[layer, p, turn], along_z(nc))

    def sum_sent(layer):
        ref = sums.at[layer, pl.ds(0, 2), pl.ds(0, 2)]
        return send(ref, ref, ms.at[layer], mr.at[layer, 0, 0], along_z(nc))

    def cur_copies(layer, p, b):
        for slot in others:
            if slot == split:
                for columns, d in ((left, -half), (right, half)):
                    ref = cur.at[layer, p, b, :, columns]
                    yield send(ref, ref, bs.at[layer], br.at[layer, p, b], along_z(d))
            else:
                ref = cur.at[layer, p, b]
                yield send(ref, ref, bs.at[layer], br.at[layer, p, b], along_z(here - slot))

    def cur_got(layer, p, b):
        ref = cur.at[layer, p, b]
        return send(ref, ref, bs.at[layer], br.at[layer, p, b], along_z(1))

    def cur_sent(layer):
        ref = cur.at[layer, pl.ds(0, 2), most]
        return send(ref, ref, bs.at[layer], br.at[layer, 0, 0], along_z(1))

    def squares_copy(p, to):
        ref = squares_row.at[p, c]
        return send(ref, ref, ns.at[0], nr.at[p], {"ra": z, "cb": to})

    def squares_got(p):
        ref = squares_row.at[p, most]
        return send(ref, ref, ns.at[0], nr.at[p], along_c(1))

    def squares_sent():
        ref = squares_row.at[pl.ds(0, 2), most]
        return send(ref, ref, ns.at[0], nr.at[0], along_c(1))

    def inverse_copy(p, b, slot):
        ref = inverse_row.at[p, b]
        return send(ref, ref, vs.at[0], vr.at[p, b], along_z(here - slot))

    def inverse_got(p, b):
        ref = inverse_row.at[p, b]
        return send(ref, ref, vs.at[0], vr.at[p, b], along_z(1))

    def inverse_sent():
        ref = inverse_row.at[pl.ds(0, 2), most]
        return send(ref, ref, vs.at[0], vr.at[0, 0], along_z(1))

    def near_first(i):
        return (2 * lax.rem(i, 2) - 1) * ((i + 1) // 2)

    side_c = 1 - 2 * lax.rem(c, 2)
    far_c = (4, 5, 3, 2, 6, 7, 1) if nc == 8 else tuple(range(nc - 1, 0, -1))

    def finish(layer, p, total):
        if layer == 0:
            own = tok[pl.ds(pl.multiple_of((p * nc + mine) * blk, blk), blk), :].astype(f32)
        else:
            own = cur[layer - 1, p, mine].astype(f32)
        new = (residual_weight * own + down_scale[layer : layer + 1, :] * total).astype(bf16)
        if layer == layers - 1:
            wide = new.astype(f32)
            squares_row[p, c] = as_row(jnp.sum(wide * wide, axis=1, keepdims=True))
            for k in far_c:
                squares_copy(p, lax.rem(c + side_c * k + nc, nc)).start()
        cur[layer, p, mine] = new
        for copy in cur_copies(layer, p, mine):
            copy.start()

    for layer in range(layers):
        if layer == 0:
            small[0].wait()
            small[1].wait()
            take_in(0)
            before = None
            for p in range(2):
                y = partials(tok[p * nc * blk : (p + 1) * nc * blk, :].astype(f32), 0).reshape(nc, blk, 2 * ffp)
                part[0, p] = y.astype(bf16)
                ends = y[:, blk - halo :, :].astype(bf16)
                if p > 0:
                    part_halo[0, p, 0] = before
                for b in range(1, nc):
                    part_halo[0, p, b] = ends[b - 1]
                before = ends[nc - 1]
                if p == 0:
                    pl.semaphore_wait(barrier, len(peers))
                    greet(0)
                for k in far_c:
                    to = lax.rem(c + side_c * k + nc, nc)
                    part_copy(0, p, to).start()
                    halo_copy(0, p, to).start()
        else:
            for p in range(2):
                if p == 0:

                    @pl.when(c != 0)
                    def _(layer=layer):
                        halo_copy(layer, 0, 0).start()

                def two_blocks(i, carry, layer=layer, p=p):
                    b0 = lax.rem(z + near_first(2 * i) + nz, nc)
                    b1 = lax.rem(z + near_first(2 * i + 1) + nz, nc)

                    @pl.when(i > 0)
                    def _():
                        cur_got(layer - 1, p, b0).wait_recv()

                    cur_got(layer - 1, p, b1).wait_recv()
                    x = jnp.concatenate([cur[layer - 1, p, b0], cur[layer - 1, p, b1]], axis=0)
                    y = partials(x.astype(f32), layer)
                    for b, first in ((b0, 0), (b1, blk)):
                        part[layer, p, b] = y[first : first + blk, :].astype(bf16)

                        @pl.when(b != c)
                        def _(b=b):
                            part_copy(layer, p, b).start()

                        ends = y[first + blk - halo : first + blk, :].astype(bf16)
                        after = lax.rem(b + 1, nc)

                        @pl.when(after != 0)
                        def _(after=after, ends=ends):
                            part_halo[layer, p, after] = ends

                            @pl.when(after != c)
                            def _():
                                halo_copy(layer, p, after).start()

                        if p == 0:

                            @pl.when(after == 0)
                            def _(ends=ends):
                                part_halo[layer, 1, 0] = ends

                                @pl.when(c != 0)
                                def _():
                                    halo_copy(layer, 1, 0).start()

                    return carry

                lax.fori_loop(0, nc // 2, two_blocks, 0)

        if layer == 0:
            take_down(0)
            greeted(0)
            greet(1)
            for load in small[2:]:
                load.wait()
            greeted(1)
            greet(2)
        for p in range(2):
            got[layer, p, c] = part[layer, p, c]
            got_halo[layer, p, c] = part_halo[layer, p, c]
            part_got(layer, p).wait_recv()
            halo_got(layer, p).wait_recv()
            for buf, count, at in ((got_halo, halo, 8 - halo), (got, blk, 8)):
                total = buf[layer, p, 0].astype(f32)
                for src in range(1, nc):
                    total = total + buf[layer, p, src].astype(f32)
                squares = jnp.sum(total[:, ff : ff + 3], axis=1, keepdims=True)
                inverse = lax.rsqrt(squares / model_width + epsilon)
                pre[p, at : at + count, 0:ff] = inverse * gate_scale[layer : layer + 1, :] * total[:, 0:ff]
                pre[p, at : at + count, ffp : ffp + ff] = (
                    inverse * value_scale[layer : layer + 1, :] * total[:, ffp : ffp + ff]
                )
            convs = []
            for lane, tap_weights in ((0, conv_gate), (ffp, conv_value)):
                y = None
                for k in range(taps):
                    at = 8 - halo + k
                    term = pre[p, at : at + blk, lane : lane + ff] * tap_weights[k, layer : layer + 1, :]
                    y = term if y is None else y + term
                convs.append(y)
            hid[layer, p, c, :, 0:ff] = (jax.nn.gelu(convs[0], approximate=True) * convs[1]).astype(bf16)
            for k in far_c:
                hid_copy(layer, p, c, lax.rem(c + side_c * k + nc, nc)).start()

        for p in range(2):

            def two_downs(i, carry, layer=layer, p=p):
                b0 = lax.rem(c + side_c * near_first(2 * i) + nc, nc)
                b1 = lax.rem(c + side_c * near_first(2 * i + 1) + nc, nc)

                @pl.when(i > 0)
                def _():
                    hid_copy(layer, p, b0, c).wait_recv()

                hid_copy(layer, p, b1, c).wait_recv()
                h = jnp.concatenate([hid[layer, p, b0], hid[layer, p, b1]], axis=0)
                d = jnp.dot(h, w_down[layer], preferred_element_type=f32).astype(bf16)
                for b, first in ((b0, 0), (b1, blk)):
                    down_part[layer, p, b] = d[first : first + blk, :]
                    slot = slot_of(b)

                    @pl.when(jnp.logical_and(slot != here, slot != split))
                    def _(b=b, slot=slot):
                        win_copy(layer, p, b, slot).start()

                    @pl.when(slot == split)
                    def _(b=b):
                        for copy in win_halves(layer, p, b):
                            copy.start()

                return carry

            lax.fori_loop(0, nc // 2, two_downs, 0)
        if layer + 1 < layers:
            take_in(layer + 1)
            take_down(layer + 1)

        for p in range(2):
            win[layer, p, here] = down_part[layer, p, mine]
            win_got(layer, p).wait_recv()
            total = win[layer, p, 0].astype(f32)
            for slot in range(1, nc):
                total = total + win[layer, p, slot].astype(f32)
            sums[layer, p, 0] = total.astype(bf16)
            if layer == 0 and p == 0:
                greeted(2)
            for copy in sum_copies(layer, p, 0):
                copy.start()
        for turn in range(2):
            for p in range(2):
                sum_got(layer, p, turn).wait_recv()
                both = sums[layer, p, 2 * turn].astype(f32) + sums[layer, p, 2 * turn + 1].astype(f32)
                if turn == 0:
                    sums[layer, p, 2] = both.astype(bf16)
                    for copy in sum_copies(layer, p, 1):
                        copy.start()
                else:
                    finish(layer, p, both)

    for p in range(2):
        squares_got(p).wait_recv()
        total = squares_row[p, 0]
        for k in range(1, nc):
            total = total + squares_row[p, k]
        inverse_row[p, mine] = lax.rsqrt(total / model_width + epsilon)
        for slot in others:
            inverse_copy(p, mine, slot).start()

    last = layers - 1

    def out_copy(p, b):
        there = pl.ds(pl.multiple_of((p * nc + b) * blk, blk), blk)
        return pltpu.make_async_copy(result.at[p, b], out.at[there], out_sem.at[0])

    for p in range(2):

        def put_block(i, carry, p=p):
            b = lax.rem(z + near_first(i) + nz, nc)

            @pl.when(i > 0)
            def _():
                cur_got(last, p, b).wait_recv()
                inverse_got(p, b).wait_recv()

            scale = as_column(inverse_row[p, b], blk)
            wide = cur[last, p, b].astype(f32) * scale * gains[layers : layers + 1, :]
            result[p, b] = wide.astype(bf16)
            out_copy(p, b).start()
            return carry

        lax.fori_loop(0, nc, put_block, 0)

    for layer in range(layers):
        for sent in (part_sent, halo_sent, hid_sent, win_sent, sum_sent, cur_sent):
            sent(layer).wait_send()
    squares_sent().wait_send()
    inverse_sent().wait_send()
    pltpu.make_async_copy(out, out, out_sem.at[0]).wait()


def on_device(
    tokens,
    norm_gains,
    gate_weight,
    value_weight,
    gate_scale,
    value_scale,
    conv_gate,
    conv_value,
    down_weight,
    down_scale,
):
    nz, nc = lax.axis_size("ra"), lax.axis_size("cb")
    rows, width = tokens.shape
    layers, _, ff = gate_weight.shape
    taps = conv_gate.shape[1]
    ffp = (ff + 3 + 127) // 128 * 128
    blk = rows // (2 * nc)
    owners = nz // nc
    dims = (layers, nz, nc, width, ff, ffp, blk, taps)
    dma = pltpu.SemaphoreType.DMA
    operands = (
        tokens,
        norm_gains,
        gate_weight.swapaxes(1, 2),
        value_weight.swapaxes(1, 2),
        gate_scale,
        value_scale,
        conv_gate.swapaxes(0, 1),
        conv_value.swapaxes(0, 1),
        down_weight,
        down_scale,
    )
    small = [operands[k] for k in (0, 1, 4, 5, 6, 7, 9)]
    return pl.pallas_call(
        functools.partial(kernel, dims),
        out_shape=jax.ShapeDtypeStruct((rows, width), bf16),
        in_specs=[pl.BlockSpec(memory_space=pltpu.HBM)] * len(operands),
        out_specs=pl.BlockSpec(memory_space=pltpu.HBM),
        scratch_shapes=[pltpu.VMEM(a.shape, a.dtype) for a in small]
        + [
            pltpu.VMEM((layers, 2, ffp, width), f32),
            pltpu.VMEM((layers, ff, width), f32),
            pltpu.VMEM((2 * ffp, width), bf16),
            pltpu.VMEM((layers - 1, width, 2 * ffp), bf16),
            pltpu.VMEM((layers, ffp, width), bf16),
            pltpu.VMEM((layers, 2, nc, blk, 2 * ffp), bf16),
            pltpu.VMEM((layers, 2, nc, taps - 1, 2 * ffp), bf16),
            pltpu.VMEM((layers, 2, nc, blk, 2 * ffp), bf16),
            pltpu.VMEM((layers, 2, nc, taps - 1, 2 * ffp), bf16),
            pltpu.VMEM((2, 8 + blk, 2 * ffp), f32),
            pltpu.VMEM((layers, 2, nc, blk, ffp), bf16),
            pltpu.VMEM((layers, 2, nc, blk, width), bf16),
            pltpu.VMEM((layers, 2, nc, blk, width), bf16),
            pltpu.VMEM((layers, 2, owners, blk, width), bf16),
            pltpu.VMEM((layers, 2, nc, blk, width), bf16),
            pltpu.VMEM((2, nc, 1, 128), f32),
            pltpu.VMEM((2, nc, 1, 128), f32),
            pltpu.VMEM((2, nc, blk, width), bf16),
            dma((len(small),)),
            dma((layers, 3)),
        ]
        + [dma((layers,)), dma((layers, 2))] * 2
        + [dma((layers,)), dma((layers, 2, nc))]
        + [dma((layers,)), dma((layers, 2)), dma((layers,)), dma((layers, 2, 2))]
        + [dma((layers,)), dma((layers, 2, nc))]
        + [dma((1,)), dma((2,)), dma((1,)), dma((2, nc)), dma((1,))]
        + [pltpu.SemaphoreType.REGULAR((3,))],
        compiler_params=pltpu.CompilerParams(
            collective_id=0, has_side_effects=True, vmem_limit_bytes=61 * 2**20
        ),
        cost_estimate=pl.CostEstimate(flops=4 * 10**8, bytes_accessed=10**7, transcendentals=0),
    )(*operands)


def solution(mesh):
    in_specs = (
        P("grp", "cb"),
        P(None, "cb"),
        P(None, "cb", "ra"),
        P(None, "cb", "ra"),
        P(None, "ra"),
        P(None, "ra"),
        P(None, None, "ra"),
        P(None, None, "ra"),
        P(None, "ra", "cb"),
        P(None, "cb"),
    )
    out_specs = P("grp", "cb")
    return jax.shard_map(on_device, mesh=mesh, in_specs=in_specs, out_specs=out_specs, check_vma=False)
```
